512 devices in a mesh: sp: 32 (over z, core), tp: 16 (over y, x).
Axes of the slice: x: 4, y: 4, z: 16, core: 2. Of those that a mesh axis runs over, the one named last changes fastest.
Arguments:
- pool_in: bfloat16 [512, 12288], P('tp', 'sp'), may hold values from -8 to 8
- doc_ids: int32 [12288], P('sp'), may hold values from 0 to 15, never falling along the last dimension, each value on 1 to 1536 neighbouring positions
- pool_map: bfloat16 [8, 64, 64], replicated, may hold values from -0.75 to 0.75
- pool_scale: float32 [512], replicated, may hold values from 0.1 to 1.9
- w_out: bfloat16 [512, 2048], P(None, 'tp'), may hold values from -0.25 to 0.25
- gate_logit: bfloat16 [12288, 2048], P('sp', 'tp'), may hold values from -8 to 8
- residual: bfloat16 [12288, 2048], P('sp', 'tp'), may hold values from -4 to 4
- first_gain: float32 [2048], P('tp'), may hold values from 0.1 to 1.9
- first_bias: float32 [2048], P('tp'), may hold values from -1.5 to 1.5
- routes: int32 [12288, 2], P('sp'), may hold values from 0 to 31, all different within a row; in each aligned block of 384 rows (0 to 383, 384 to 767, ...) at most 48 rows name the same one
- route_weight: float32 [12288, 2], P('sp'), may hold values from 0.25 to 1
- w_gate: bfloat16 [32, 2048, 1024], P('sp', None, 'tp'), may hold values from -0.125 to 0.125
- w_up: bfloat16 [32, 2048, 1024], P('sp', None, 'tp'), may hold values from -0.125 to 0.125
- w_down: bfloat16 [32, 1024, 2048], P('sp', None, 'tp'), may hold values from -0.375 to 0.375
- second_gain: float32 [2048], P('tp'), may hold values from 0.1 to 1.9
- second_bias: float32 [2048], P('tp'), may hold values from -1.5 to 1.5
Outputs:
- layer_out: bfloat16 [12288, 2048], P('sp', 'tp')
The draws below stay inside these ranges and needn't reach their ends.
Inputs may be any that keep to these rules, and one draw needn't show every extreme that they name: `doc_ids`: never falling; each document spans 1 to 1536 positions. `routes`: each row names 2 different experts; in each aligned block of 384 rows (the rows of one index of sp) no expert is named by more than 48 rows, a bound that some block reaches.
All inputs are finite; a program needn't handle non-finite values.
Results may differ from the reference program's by a relative error of at most 0.008.
Values may be sent and summed in bfloat16 or wider, within the bound.
A program may use at most 64 MiB of HBM per device.

```python
import math
import jax
import jax.numpy as jnp
import numpy as np
from jax import lax

D = 2048
MIX_W = 512
GROUP_W = 64
GROUPS = 8
DE = 1024
TOPK = 2
TOK_DEV = 384
TOKENS = 12288
EXPERTS = 32
CAP = 48
DOCS = 16
DOC_MOST = 1536
N_SP = 32


def draw_pool_in(key, part):
    walk_key, rough_key = jax.random.split(jax.random.fold_in(key, 7))
    blocks = TOKENS // 16
    drift_walk = jnp.cumsum(jax.random.normal(walk_key, (MIX_W, blocks), jnp.float32), axis=1)
    drift_walk = drift_walk / jnp.sqrt(jnp.float32(blocks))
    smooth = jnp.repeat(drift_walk, 16, axis=1)
    rough_part = jax.random.normal(rough_key, (MIX_W, TOKENS), jnp.float32)
    return jnp.clip(0.8 * rough_part + smooth, -8.0, 8.0).astype(jnp.bfloat16)


def level_of(own_key, shape, shards, least, top_value):
    loudness = 1.0
    for dim, blocks in shards:
        steps = jax.random.uniform(jax.random.fold_in(jax.random.fold_in(own_key, 6), dim), (blocks,), jnp.float32, least / len(shards), top_value / len(shards))
        loudness = loudness * jnp.repeat(jnp.exp(steps), shape[dim] // blocks).reshape((-1,) + (1,) * (len(shape) - 1 - dim))
    return loudness


def length_profile(amount, total, limit, lean):
    portions = [(1 << 20) // math.isqrt(standing ** lean) + 1 for standing in range(2, amount + 1)]
    spare, holding = total - limit - (amount - 1), [1] * (amount - 1)
    while spare > 0:
        candidates = [i for i in range(amount - 1) if holding[i] < limit]
        whole, left = sum([portions[i] for i in candidates]), spare
        for i in candidates:
            addition = min(limit - holding[i], max(1, left * portions[i] // whole), spare)
            holding[i] = holding[i] + addition
            spare = spare - addition
    return np.array([limit] + holding)


def uneven(rng, number_of, total, bound, lean):
    if number_of == 2:
        one = jax.random.randint(rng, (), max(1, total - bound), min(bound, total - 1) + 1)
        return jnp.stack([one, total - one])
    lengths = jnp.asarray(length_profile(number_of, total, bound, lean), jnp.int32)
    twos = (number_of - 1) // 2
    giver, receiver = lengths[1:1 + 2 * twos:2], lengths[2:2 + 2 * twos:2]
    room = jnp.minimum(giver - 1, bound - receiver)
    passed = jax.random.randint(jax.random.fold_in(rng, 1), (twos,), 0, 1 << 20) % (room + 1)
    lengths = lengths.at[1:1 + 2 * twos:2].set(giver - passed).at[2:2 + 2 * twos:2].set(receiver + passed)
    return lengths[jax.random.permutation(jax.random.fold_in(rng, 2), number_of)]


def routed_block(stream_key, own, number, rows, amount, top, most, slope):
    order = jax.random.permutation(stream_key, amount)
    crowded, ordinary = portions_of(amount, rows * top, most, slope, True), portions_of(amount, rows * top, most, slope, False)
    places = jnp.arange(amount)

    def named(lengths, rotation):
        used = int((lengths > 0).sum())
        fixed = max(1, used // 4)
        shifted = fixed + (places - fixed + rotation * (used - fixed)) % max(1, amount - fixed)
        return jnp.zeros((amount,), jnp.int32).at[order[jnp.where(places < fixed, places, shifted)]].set(jnp.asarray(lengths, jnp.int32))

    lengths = jnp.where(number % 4 == 0, named(crowded, number // 4), named(ordinary, number - number // 4 - 1))
    mixed = jax.random.permutation(jax.random.fold_in(own, 3), amount)
    donor, receiver = mixed[0:amount // 2 * 2:2], mixed[1:amount // 2 * 2:2]
    slack = jnp.minimum(lengths[donor] - 1, most - lengths[receiver]) // 2
    slack = jnp.where((donor == order[0]) | (receiver == order[0]) | (lengths[receiver] == 0), 0, jnp.maximum(slack, 0))
    shifted = jax.random.randint(jax.random.fold_in(own, 4), (amount // 2,), 0, 1 << 20) % (slack + 1)
    lengths = lengths.at[donor].add(-shifted).at[receiver].add(shifted)
    labels = jnp.searchsorted(jnp.cumsum(lengths), jnp.arange(rows * top), side="right").astype(jnp.int32)
    grid = labels.reshape(top, rows).T
    grid = grid[jax.random.permutation(jax.random.fold_in(own, 1), rows)]
    rotation = jax.random.randint(jax.random.fold_in(own, 2), (rows, 1), 0, top)
    return jnp.take_along_axis(grid, (jnp.arange(top)[None, :] + rotation) % top, axis=1)


def portions_of(amount, total, limit, slope, full):
    loads = [(1 << 20) // math.isqrt(rank ** slope) + 1 for rank in range(1, amount + 1)]
    largest = limit if full else min(limit, max(-(-total // amount), total * loads[0] // sum(loads)))
    least = 1 if total - largest >= amount - 1 else 0
    holding, spare = [largest] + [least] * (amount - 1), total - largest - least * (amount - 1)
    while spare > 0:
        candidates = [i for i in range(1, amount) if holding[i] < largest] or [i for i in range(1, amount) if holding[i] < limit]
        pool, left = sum([loads[i] for i in candidates]), spare
        for i in candidates:
            more = min(limit - holding[i], max(1, left * loads[i] // pool), spare)
            holding[i] = holding[i] + more
            spare = spare - more
    return np.array(holding)


def gaussian(rng, extent, deviation, limit, cuts=(), held_as=jnp.bfloat16):
    loudness = level_of(rng, extent, cuts, -0.22, 0.18) if cuts else 1.0
    entries = jax.random.normal(rng, extent, jnp.float32) * deviation * loudness
    return jnp.minimum(jnp.maximum(entries, -limit), limit).astype(held_as)


def setup_inputs(seed: int = 0) -> dict:
    arg_keys = jax.random.split(jax.random.key(seed), 17)
    pool_in = draw_pool_in(jax.random.fold_in(arg_keys[16], 71), 0)
    doc_ids = jnp.searchsorted(jnp.cumsum(uneven(arg_keys[1], DOCS, TOKENS, DOC_MOST, 1)), jnp.arange(TOKENS), side="right").astype(jnp.int32)
    pool_map = gaussian(arg_keys[2], (GROUPS, GROUP_W, GROUP_W), GROUP_W ** -0.5, 0.75)
    pool_scale = jnp.clip(1.0 + 0.18 * jax.random.normal(arg_keys[3], (MIX_W,), jnp.float32), 0.1, 1.9)
    w_out = gaussian(arg_keys[4], (MIX_W, D), MIX_W ** -0.5, 0.25, ((1, 16),))
    gate_logit = gaussian(arg_keys[5], (TOKENS, D), 1.5, 8.0, ((0, 32), (1, 16)))
    residual = gaussian(arg_keys[6], (TOKENS, D), 0.6, 4.0, ((0, 32), (1, 16)))
    first_gain = jnp.clip(1.0 + 0.18 * jax.random.normal(arg_keys[7], (D,), jnp.float32), 0.1, 1.9)
    first_bias = gaussian(arg_keys[8], (D,), 0.3, 1.5, ((0, 16),), jnp.float32)
    routes_keys = jax.random.split(jax.random.fold_in(arg_keys[9], 1), TOKENS // TOK_DEV)
    routes_turns = jax.random.permutation(jax.random.fold_in(arg_keys[9], 3), TOKENS // TOK_DEV)
    routes = jax.vmap(lambda own, number: routed_block(jax.random.fold_in(arg_keys[9], 2), own, number, TOK_DEV, EXPERTS, TOPK, CAP, 1))(routes_keys, routes_turns).reshape((TOKENS, TOPK))
    route_weight = jnp.clip(0.25 + 0.75 * jax.random.uniform(arg_keys[10], (TOKENS, TOPK), jnp.float32) ** level_of(arg_keys[10], (TOKENS, TOPK), ((0, 32),), -0.2, 0.2), 0.25, 1.0)
    w_gate = gaussian(arg_keys[11], (EXPERTS, D, DE), D ** -0.5, 0.125, ((0, 32), (2, 16)))
    w_up = gaussian(arg_keys[12], (EXPERTS, D, DE), D ** -0.5, 0.125, ((0, 32), (2, 16)))
    w_down = gaussian(arg_keys[13], (EXPERTS, DE, D), (DE // 4) ** -0.5, 0.375, ((0, 32), (2, 16)))
    second_gain = jnp.clip(1.0 + 0.18 * jax.random.normal(arg_keys[14], (D,), jnp.float32), 0.1, 1.9)
    second_bias = gaussian(arg_keys[15], (D,), 0.3, 1.5, ((0, 16),), jnp.float32)
    return dict(pool_in=pool_in, doc_ids=doc_ids, pool_map=pool_map, pool_scale=pool_scale, w_out=w_out, gate_logit=gate_logit, residual=residual, first_gain=first_gain, first_bias=first_bias, routes=routes, route_weight=route_weight, w_gate=w_gate, w_up=w_up, w_down=w_down, second_gain=second_gain, second_bias=second_bias)


EPS = 1e-05
ALPHA = 8.0 ** 0.25

def layer_norm(row_data, gain_vec, bias_vec):
    row_mean = lax.optimization_barrier(jnp.mean(row_data, axis=1, keepdims=True))
    row_var = lax.optimization_barrier(jnp.mean(row_data * row_data, axis=1, keepdims=True)) - row_mean * row_mean
    return (row_data - row_mean) * lax.rsqrt(row_var + EPS) * gain_vec + bias_vec

def pool_scales(pool_in, doc_ids):
    values = pool_in.astype(jnp.float32)
    length = values.shape[1]
    opening = jnp.concatenate([jnp.ones((1,), bool), doc_ids[1:] != doc_ids[:-1]])
    places = jnp.arange(length, dtype=jnp.int32)
    doc_start = lax.cummax(jnp.where(opening, places, 0), axis=0)
    prefix = jnp.concatenate([jnp.zeros((MIX_W, 1), jnp.float32), jnp.cumsum(values, axis=1)], axis=1)
    upper_at = places + 1
    group_id = jnp.arange(MIX_W, dtype=jnp.int32) // GROUP_W
    doc_mask = (group_id % 2 == 1)[:, None]
    window = jnp.left_shift(2, group_id // 2 % 4)[:, None]
    lower_at = jnp.where(doc_mask, doc_start[None, :], jnp.maximum(upper_at[None, :] - window, doc_start[None, :]))
    lower_at = lower_at.astype(jnp.int32)
    window_sum = prefix[:, 1:] - jnp.take_along_axis(prefix, lower_at, axis=1)
    counted = (upper_at[None, :] - lower_at).astype(jnp.float32)
    return (window_sum / counted - values).astype(jnp.bfloat16)

def reference(pool_in, doc_ids, pool_map, pool_scale, w_out, gate_logit, residual, first_gain, first_bias, routes, route_weight, w_gate, w_up, w_down, second_gain, second_bias):
    pooled = pool_scales(pool_in, doc_ids)
    grouped = jnp.einsum('gct,gcd->tgd', pooled.reshape(GROUPS, GROUP_W, TOKENS).astype(jnp.float32), pool_map.astype(jnp.float32))
    mapped = (grouped.reshape(TOKENS, MIX_W) * pool_scale).astype(jnp.bfloat16)
    mixer_out = jnp.dot(mapped, w_out, preferred_element_type=jnp.float32) * jax.nn.sigmoid(gate_logit.astype(jnp.float32))
    normed = layer_norm(ALPHA * residual.astype(jnp.float32) + mixer_out, first_gain, first_bias).astype(jnp.bfloat16)
    flat_routes = routes.reshape(-1).astype(jnp.int32)
    one_hot = (flat_routes[:, None] == jnp.arange(EXPERTS, dtype=jnp.int32)[None, :]).astype(jnp.int32)
    slot_rank = lax.optimization_barrier(jnp.sum((jnp.cumsum(one_hot, axis=0, dtype=jnp.int32) - 1) * one_hot, axis=1)).astype(jnp.int32)
    rows_most = N_SP * CAP
    token_of = jnp.arange(TOKENS * TOPK, dtype=jnp.int32) // TOPK
    flat_weight = route_weight.reshape(-1)

    def one_expert(running, expert):
        slot_ids = jnp.where(flat_routes == expert, slot_rank, rows_most).astype(jnp.int32)
        picked = jnp.zeros((rows_most,), jnp.int32).at[slot_ids].set(token_of, mode='drop')
        slot_weight = jnp.zeros((rows_most,), jnp.float32).at[slot_ids].set(flat_weight, mode='drop')
        inputs = normed[picked]
        gate_part = jnp.dot(inputs, w_gate[expert], preferred_element_type=jnp.float32)
        up_part = jnp.dot(inputs, w_up[expert], preferred_element_type=jnp.float32)
        hidden = (jax.nn.silu(gate_part) * up_part).astype(jnp.bfloat16)
        result = jnp.dot(hidden, w_down[expert], preferred_element_type=jnp.float32).astype(jnp.bfloat16)
        return (running.at[picked].add(slot_weight[:, None] * result.astype(jnp.float32)), None)
    moe_sum, _ = lax.scan(one_expert, jnp.zeros((TOKENS, D), jnp.float32), jnp.arange(EXPERTS, dtype=jnp.int32))
    return layer_norm(ALPHA * normed.astype(jnp.float32) + moe_sum, second_gain, second_bias).astype(jnp.bfloat16)
```

```python
import functools

import jax
import jax.numpy as jnp
from jax import lax
from jax.experimental import pallas as pl
from jax.experimental.pallas import tpu as pltpu
from jax.sharding import Mesh
from jax.sharding import PartitionSpec as P

MESH = pl.DeviceIdType.MESH
F32 = jnp.float32
BF16 = jnp.bfloat16
TP = ("y", "x")
EPS = 1e-05
ALPHA = 8.0**0.25
NZ, NC, NY, NX = 16, 2, 4, 4
NTP = NY * NX
EXPERTS = NZ * NC
CAP = 48
TOK = 384
MIX_W = 512
FEAT = 2048
FD = 128
HD = 64
LANE = 128
CHUNKS = TOK // LANE
BACK = 4
NG = NZ // NY
PIECES = NG * NC * NY
ORDER = (2, 1, 3, 0)


def dot(a, b, dims=((1,), (0,))):
    return lax.dot_general(a, b, (dims, ((), ())), preferred_element_type=F32)


def iota(shape, dim):
    return lax.broadcasted_iota(jnp.int32, shape, dim)


def turned(row):
    return jnp.broadcast_to(row, (LANE, LANE)).T


def part(value, k):
    return value[:, k * LANE : (k + 1) * LANE]


def rows_of(value, k):
    return value[k * LANE : (k + 1) * LANE]


def remote(src, dst, send, recv, where):
    return pltpu.make_async_remote_copy(
        src_ref=src, dst_ref=dst, send_sem=send, recv_sem=recv, device_id=where, device_id_type=MESH
    )


def norm_columns(totals):
    mean = totals[0:1] / FEAT
    var = totals[1:2] / FEAT - mean * mean
    return mean, lax.rsqrt(var + EPS)


def layer_kernel(
    pool_ref,
    ids_ref,
    pmap_ref,
    scale_ref,
    wout_ref,
    gate_ref,
    res_ref,
    gain1_ref,
    bias1_ref,
    routes_ref,
    rweight_ref,
    wg_hbm,
    wu_hbm,
    wd_hbm,
    gain2_ref,
    bias2_ref,
    out_ref,
    wg_v,
    wu_v,
    halo,
    pk,
    pk_in,
    pg,
    st1,
    st2,
    slots,
    send_rows,
    xb,
    wb,
    db,
    acc,
    hb,
    ob,
    rb,
    pick,
    nat,
    load_sem,
    halo_s,
    halo_r,
    pk_s,
    pk_r,
    pg_s,
    pg_r,
    st1_s,
    st1_r,
    st2_s,
    st2_r,
    disp_s,
    disp_r,
    xf_s,
    xf_r,
    w_s,
    w_r,
    h_s,
    h_r,
    ret_s,
    ret_r,
):
    z, c, y, x = (lax.axis_index(name) for name in ("z", "core", "y", "x"))
    here = (z, c, y, x)
    sp = z * NC + c
    tp = y * NX + x
    right, left = lax.rem(x + 1, NX), lax.rem(x + NX - 1, NX)
    across = lax.rem(x + 2, NX)
    down, up = lax.rem(y + 1, NY), lax.rem(y + NY - 1, NY)
    beyond = lax.rem(y + 2, NY)
    own_piece = (z // NY) * NC * NY + c * NY + y
    shift = lax.rem(y - z + NZ, NY)
    own_self = lax.rem(2 * z, NY) == y

    def sp_device(k):
        return (k // NC, lax.rem(k, NC), y, x)

    def plane_device(k):
        return (z, c, k // NX, lax.rem(k, NX))

    def expert_device(e):
        ze = e // NC
        return (ze, lax.rem(e, NC), lax.rem(z + ze, NY), x)

    def source_device(p):
        g = p // (NC * NY)
        return (g * NY + shift, lax.rem(p // NY, NC), lax.rem(p, NY), x)

    barrier = pltpu.get_barrier_semaphore()

    def greet(device):
        pl.semaphore_signal(barrier, inc=1, device_id=device, device_id_type=MESH)

    @pl.loop(0, NTP)
    def _(k):
        @pl.when(k != tp)
        def _():
            greet(plane_device(k))

    @pl.loop(0, EXPERTS)
    def _(e):
        @pl.when(jnp.logical_not(jnp.logical_and(own_self, e == sp)))
        def _():
            greet(expert_device(e))

    @pl.loop(0, PIECES)
    def _(p):
        @pl.when(jnp.logical_not(jnp.logical_and(own_self, p == own_piece)))
        def _():
            greet(source_device(p))

    for b in range(1, BACK + 1):

        @pl.when(sp + b < EXPERTS)
        def _():
            greet(sp_device(sp + b))

        @pl.when(sp >= b)
        def _():
            greet(sp_device(sp - b))

    loads = [
        pltpu.make_async_copy(wg_hbm, wg_v, load_sem.at[0]),
        pltpu.make_async_copy(wu_hbm, wu_v, load_sem.at[1]),
        pltpu.make_async_copy(wd_hbm, db.at[y], load_sem.at[2]),
    ]
    for load in loads:
        load.start()

    ids = ids_ref[...].astype(F32)
    pool = pool_ref[...]
    last_id = ids[:, TOK - 1 : TOK]
    tail = jnp.broadcast_to((ids == last_id).astype(F32), (8, TOK)).astype(BF16)
    row = iota((LANE, TOK), 0)
    padded = jnp.concatenate([pool, jnp.zeros((LANE - 32, TOK), BF16)], axis=0)
    padded = jnp.where(row == 32, jnp.ones_like(padded), padded)
    sums = dot(tail, padded, ((1,), (1,)))
    line = iota((8, LANE), 0)
    packet = jnp.where(line == 0, sums, jnp.broadcast_to(last_id, (8, LANE)))
    packet = jnp.where(line == 2, jnp.broadcast_to(part(ids, CHUNKS - 1), (8, LANE)), packet)
    pk[...] = packet

    is_doc = x >= 2
    window = jnp.where(is_doc, 4 * TOK, jnp.left_shift(2, y))
    id_col = jnp.concatenate([turned(part(ids, k)) for k in range(CHUNKS)], axis=0)
    sum_own, count_own = [], []
    ones8 = jnp.ones((8, TOK), BF16)
    for k in range(CHUNKS):
        spos = iota((TOK, LANE), 0)
        tpos = iota((TOK, LANE), 1) + k * LANE
        gap = tpos - spos
        keep = (id_col == part(ids, k)) & (gap >= 0) & (gap < window)
        mask = keep.astype(F32).astype(BF16)
        sum_own.append(dot(pool, mask))
        count_own.append(dot(ones8, mask)[0:1])

    expert = iota((EXPERTS, TOK), 0).astype(F32)
    ways = []
    for k in range(2):
        column = jnp.broadcast_to(routes_ref[:, k : k + 1].astype(F32), (TOK, LANE))
        named = jnp.concatenate([rows_of(column, j).T[0:1] for j in range(CHUNKS)], axis=1)
        ways.append((expert == named).astype(F32))
    earlier = (iota((TOK, TOK), 0) < iota((TOK, TOK), 1)).astype(F32).astype(BF16)
    rank = dot((ways[0] + ways[1]).astype(BF16), earlier) + expert * CAP
    for k in range(2):
        slots[k : k + 1, :] = jnp.sum(ways[k] * rank, axis=0, keepdims=True)

    peers = NTP - 1
    partners = 2 * (EXPERTS - own_self.astype(jnp.int32))
    ahead = jnp.minimum(EXPERTS - 1 - sp, BACK)
    behind = jnp.minimum(sp, BACK)
    pl.semaphore_wait(barrier, peers + partners + ahead + behind)

    for b in range(1, BACK + 1):

        @pl.when(sp + b < EXPERTS)
        def _():
            remote(
                pk, pk_in.at[b - 1], pk_s.at[b - 1], pk_r.at[b - 1], sp_device(sp + b)
            ).start()

    edge = pool_ref.at[:, pl.ds(TOK - LANE, LANE)]

    @pl.when(sp + 1 < EXPERTS)
    def _():
        remote(edge, halo, halo_s, halo_r, sp_device(sp + 1)).start()

    wout_t = jnp.concatenate(
        [rows_of(wout_ref[...], k).astype(F32).T for k in range(MIX_W // LANE)], axis=1
    ).astype(BF16)
    gate_t = jnp.concatenate(
        [rows_of(gate_ref[...], k).astype(F32).T for k in range(CHUNKS)], axis=1
    )
    gate_t = jax.nn.sigmoid(gate_t)
    res_t = ALPHA * jnp.concatenate(
        [rows_of(res_ref[...], k).astype(F32).T for k in range(CHUNKS)], axis=1
    )
    none = jnp.zeros((HD, HD), F32)
    maps = []
    for k in range(MIX_W // LANE):
        upper = jnp.concatenate([pmap_ref[2 * k].astype(F32), none], axis=1)
        lower = jnp.concatenate([none, pmap_ref[2 * k + 1].astype(F32)], axis=1)
        maps.append(jnp.concatenate([upper, lower], axis=0).T.astype(BF16))
    scales = [turned(part(scale_ref[...], k)) for k in range(MIX_W // LANE)]
    gain1 = turned(gain1_ref[...])
    bias1 = turned(bias1_ref[...])

    @pl.when(sp >= 1)
    def _():
        remote(edge, halo, halo_s, halo_r, here).wait_recv()

    for b in range(1, BACK + 1):

        @pl.when(sp >= b)
        def _():
            remote(pk, pk_in.at[b - 1], pk_s.at[b - 1], pk_r.at[b - 1], here).wait_recv()

    first_id = jnp.broadcast_to(ids[:, 0:1], (1, LANE))
    carry = jnp.zeros((1, LANE), F32)
    for b in range(1, BACK + 1):
        found = pk_in[b - 1]
        same = (found[1:2] == first_id) & (jnp.broadcast_to(sp, (1, LANE)) >= b)
        carry = carry + jnp.where(same, found[0:1], 0.0)
    carry_col = turned(carry)
    doc_flag = is_doc.astype(F32)
    halo_on = jnp.broadcast_to(jnp.logical_and(sp >= 1, x < 2), (LANE, LANE))
    halo_ids = turned(pk_in[0][2:3])
    gap = iota((LANE, LANE), 1) + LANE - iota((LANE, LANE), 0)
    keep = (halo_ids == part(ids, 0)) & (gap < window) & halo_on
    mask = keep.astype(F32).astype(BF16)
    halo_in = jnp.where(halo_on[0:32], halo[...].astype(F32), 0.0).astype(BF16)
    halo_sum = dot(halo_in, mask)
    halo_count = dot(ones8[:, :LANE], mask)[0:1]
    for k in range(CHUNKS):
        head = (part(ids, k) == first_id).astype(F32) * doc_flag
        total = sum_own[k] + carry_col[0:32] * head
        count = count_own[k] + carry_col[32:33] * head
        if k == 0:
            total = total + halo_sum
            count = count + halo_count
        pooled = total / count - part(pool, k).astype(F32)
        pg[tp, :, k * LANE : (k + 1) * LANE] = pooled.astype(BF16)

    @pl.loop(1, NTP)
    def _(k):
        other = lax.rem(tp + k, NTP)
        remote(pg.at[tp], pg.at[tp], pg_s.at[other], pg_r.at[tp], plane_device(other)).start()

    loads[0].wait()
    loads[1].wait()
    loads[2].wait()
    wb[y] = jnp.concatenate([wg_v[...], wu_v[...]], axis=1)

    @pl.loop(1, NTP)
    def _(k):
        other = lax.rem(tp + k, NTP)
        remote(pg.at[tp], pg.at[other], pg_s.at[other], pg_r.at[other], here).wait_recv()

    mapped = []
    for k in range(MIX_W // LANE):
        grouped = dot(maps[k], pg[4 * k : 4 * k + 4].reshape(LANE, TOK))
        scaled = [part(grouped, j) * scales[k] for j in range(CHUNKS)]
        mapped.append(jnp.concatenate(scaled, axis=1).astype(BF16))
    mixed = res_t + dot(wout_t, jnp.concatenate(mapped, axis=0)) * gate_t
    st1[tp, 0:1] = jnp.sum(mixed, axis=0, keepdims=True)
    st1[tp, 1:2] = jnp.sum(mixed * mixed, axis=0, keepdims=True)

    @pl.loop(1, NTP)
    def _(k):
        other = lax.rem(tp + k, NTP)
        remote(st1.at[tp], st1.at[tp], st1_s.at[other], st1_r.at[tp], plane_device(other)).start()

    @pl.loop(1, NTP)
    def _(k):
        other = lax.rem(tp + k, NTP)
        remote(st1.at[tp], st1.at[other], st1_s.at[other], st1_r.at[other], here).wait_recv()

    mean, rstd = norm_columns(jnp.sum(st1[...], axis=0))
    centred = (mixed - mean) * rstd
    normed = jnp.concatenate(
        [part(centred, k) * gain1 + bias1 for k in range(CHUNKS)], axis=1
    ).astype(BF16)

    for k in range(8):
        first = k * (EXPERTS * CAP // 8)
        place = (iota((EXPERTS * CAP // 8, TOK), 0) + first).astype(F32)
        chosen = (place == slots[0:1, :]) | (place == slots[1:2, :])
        rows = dot(chosen.astype(F32).astype(BF16), normed, ((1,), (1,)))
        send_rows[4 * k : 4 * k + 4] = rows.astype(BF16).reshape(4, CAP, FD)

    for q in ORDER:

        @pl.loop(0, NY * NC)
        def _(k):
            ze = lax.rem(z - k // NC - NY * q + 2 * NZ, NZ)
            e = ze * NC + lax.rem(k, NC)

            @pl.when(jnp.logical_not(jnp.logical_and(own_self, e == sp)))
            def _():
                remote(
                    send_rows.at[e],
                    xb.at[x, z // NY, c, y],
                    disp_s.at[e],
                    disp_r.at[own_piece],
                    expert_device(e),
                ).start()

    @pl.when(own_self)
    def _():
        xb[x, z // NY, c, y] = send_rows[sp]

    def neighbour(yy):
        return (z, c, yy, x)

    def beside(xx):
        return (z, c, y, xx)

    w_own = [
        remote(wb.at[y], wb.at[y], w_s.at[0], w_r.at[0], neighbour(down)),
        remote(wb.at[y], wb.at[y], w_s.at[1], w_r.at[1], neighbour(up)),
        remote(db.at[y], db.at[y], w_s.at[2], w_r.at[2], neighbour(down)),
        remote(db.at[y], db.at[y], w_s.at[3], w_r.at[3], neighbour(up)),
    ]
    for copy in w_own:
        copy.start()

    for k in range(CHUNKS):
        nat[k * LANE : (k + 1) * LANE] = part(normed, k).astype(F32).T
        for way in range(2):
            column = turned(slots[way : way + 1, k * LANE : (k + 1) * LANE])
            for j in range(EXPERTS * CAP // LANE):
                lane = (iota((LANE, LANE), 1) + j * LANE).astype(F32)
                pick[way * TOK + k * LANE : way * TOK + (k + 1) * LANE, j * LANE : (j + 1) * LANE] = (
                    (lane == column).astype(F32).astype(BF16)
                )

    def group_of(q):
        near = lax.rem(y - 2 * z + 2 * NZ, NY)
        return lax.rem(z + near + NY * q, NZ) // NY

    xf = []
    for i, q in enumerate(ORDER):
        g = group_of(q)

        @pl.loop(0, NC * NY)
        def _(k):
            p = g * NC * NY + k

            @pl.when(jnp.logical_not(jnp.logical_and(own_self, p == own_piece)))
            def _():
                remote(
                    send_rows.at[0],
                    xb.at[x, g, k // NY, lax.rem(k, NY)],
                    disp_s.at[0],
                    disp_r.at[p],
                    here,
                ).wait_recv()

        mine = xb.at[x, g]
        to_right = remote(mine, mine, xf_s.at[0, i], xf_r.at[0, i], beside(right))
        to_left = remote(mine, mine, xf_s.at[1, i], xf_r.at[1, i], beside(left))
        to_right.start()
        to_left.start()
        xf += [to_right, to_left]
        if i == 2:
            w_own[0].wait_recv()
            w_own[1].wait_recv()
            half = FEAT // 2
            from_up = wb.at[up, pl.ds(0, half)]
            from_down = wb.at[down, pl.ds(half, half)]
            relays = [
                remote(from_up, from_up, w_s.at[4], w_r.at[4], neighbour(down)),
                remote(from_down, from_down, w_s.at[5], w_r.at[5], neighbour(up)),
            ]
            for copy in relays:
                copy.start()

    for i, q in enumerate(ORDER):
        g = group_of(q)
        xf[2 * i].wait_recv()
        xf[2 * i + 1].wait_recv()
        if i % 2 == 0:
            piece = xb.at[left, g]
            relay = remote(piece, piece, xf_s.at[2, i], xf_r.at[2, i], beside(right))
        else:
            piece = xb.at[right, g]
            relay = remote(piece, piece, xf_s.at[2, i], xf_r.at[2, i], beside(left))
        relay.start()
        xf.append(relay)

    w_own[2].wait_recv()
    w_own[3].wait_recv()
    half = EXPERTS * 16
    from_up = db.at[up, pl.ds(0, half)]
    from_down = db.at[down, pl.ds(half, half)]
    relays += [
        remote(from_up, from_up, w_s.at[6], w_r.at[6], neighbour(down)),
        remote(from_down, from_down, w_s.at[7], w_r.at[7], neighbour(up)),
    ]
    relays[2].start()
    relays[3].start()

    relays[0].wait_recv()
    relays[1].wait_recv()

    def projected(xx):
        tiles, weights = [], []
        for yy in range(NY):
            tiles.append(xb[xx, :, :, yy].reshape(TOK, FD))
            start = pl.multiple_of((yy * NX + xx) * FD, FD)
            weights.append(
                jnp.concatenate([wb[b, pl.ds(start, FD), :] for b in range(NY)], axis=1)
            )
        return dot(jnp.concatenate(tiles, axis=1), jnp.concatenate(weights, axis=0))

    acc[...] = projected(x)
    acc[...] += projected(left)
    acc[...] += projected(right)
    for i in range(NG):
        xf[2 * NG + i].wait_recv()
    acc[...] += projected(across)

    low = iota((TOK, LANE), 1) < HD
    for pair in range(NY // 2):
        one = acc[:, 2 * pair * LANE : (2 * pair + 1) * LANE]
        two = acc[:, (2 * pair + 1) * LANE : (2 * pair + 2) * LANE]
        gate = jnp.where(low, one, pltpu.roll(two, HD, 1))
        lift = jnp.where(low, pltpu.roll(one, HD, 1), two)
        hidden = gate * jax.nn.sigmoid(gate) * lift
        hb[x, :, pair * LANE : (pair + 1) * LANE] = hidden.astype(BF16)

    mine = hb.at[x]
    h_right = remote(mine, mine, h_s.at[0], h_r.at[0], beside(right))
    h_left = remote(mine, mine, h_s.at[1], h_r.at[1], beside(left))
    h_right.start()
    h_left.start()
    relays[2].wait_recv()
    relays[3].wait_recv()

    def lowered(xx):
        blocks = []
        for yy in range(NY):
            pieces = [
                db[yy, pl.ds(pl.multiple_of((b * NX + xx) * HD, HD), HD), :] for b in range(NY)
            ]
            blocks.append(jnp.concatenate(pieces, axis=0))
        return dot(hb[xx], jnp.concatenate(blocks, axis=1))

    acc[...] = lowered(x)
    half = TOK // 2
    h_right.wait_recv()
    piece = hb.at[left, pl.ds(0, half)]
    h_first = remote(piece, piece, h_s.at[2], h_r.at[2], beside(right))
    h_first.start()
    h_left.wait_recv()
    piece = hb.at[right, pl.ds(half, half)]
    h_second = remote(piece, piece, h_s.at[3], h_r.at[3], beside(left))
    h_second.start()
    acc[...] += lowered(left)
    acc[...] += lowered(right)
    h_first.wait_recv()
    h_second.wait_recv()
    result = (acc[...] + lowered(across)).astype(BF16)
    for yy in range(NY):
        ob[:, :, yy] = part(result, yy).reshape(NG, NC, CAP, FD)

    for q in ORDER:
        g = group_of(q)

        @pl.loop(0, NC * NY)
        def _(k):
            p = g * NC * NY + k

            @pl.when(jnp.logical_not(jnp.logical_and(own_self, p == own_piece)))
            def _():
                remote(
                    ob.at[g, k // NY, lax.rem(k, NY)],
                    rb.at[sp],
                    ret_s.at[p],
                    ret_r.at[sp],
                    source_device(p),
                ).start()

    @pl.when(own_self)
    def _():
        rb[sp] = ob[z // NY, c, y]

    @pl.loop(0, EXPERTS)
    def _(e):
        @pl.when(jnp.logical_not(jnp.logical_and(own_self, e == sp)))
        def _():
            remote(ob.at[0, 0, 0], rb.at[e], ret_s.at[0], ret_r.at[e], here).wait_recv()

    picked = dot(pick[...], rb[...].reshape(EXPERTS * CAP, FD))
    final = (
        ALPHA * nat[...]
        + picked[:TOK] * rweight_ref[:, 0:1]
        + picked[TOK:] * rweight_ref[:, 1:2]
    )
    for k in range(CHUNKS):
        block = rows_of(final, k).T
        st2[tp, 0:1, k * LANE : (k + 1) * LANE] = jnp.sum(block, axis=0, keepdims=True)
        st2[tp, 1:2, k * LANE : (k + 1) * LANE] = jnp.sum(block * block, axis=0, keepdims=True)

    @pl.loop(1, NTP)
    def _(k):
        other = lax.rem(tp + k, NTP)
        remote(st2.at[tp], st2.at[tp], st2_s.at[other], st2_r.at[tp], plane_device(other)).start()

    @pl.loop(1, NTP)
    def _(k):
        other = lax.rem(tp + k, NTP)
        remote(st2.at[tp], st2.at[other], st2_s.at[other], st2_r.at[other], here).wait_recv()

    mean, rstd = norm_columns(jnp.sum(st2[...], axis=0))
    for k in range(CHUNKS):
        centred = (rows_of(final, k) - turned(part(mean, k))) * turned(part(rstd, k))
        out_ref[k * LANE : (k + 1) * LANE, :] = (
            centred * gain2_ref[...] + bias2_ref[...]
        ).astype(BF16)

    for b in range(1, BACK + 1):

        @pl.when(sp + b < EXPERTS)
        def _():
            remote(pk, pk_in.at[b - 1], pk_s.at[b - 1], pk_r.at[b - 1], here).wait_send()

    @pl.when(sp + 1 < EXPERTS)
    def _():
        remote(edge, halo, halo_s, halo_r, here).wait_send()

    @pl.loop(1, NTP)
    def _(k):
        other = lax.rem(tp + k, NTP)
        remote(pg.at[tp], pg.at[tp], pg_s.at[other], pg_r.at[tp], here).wait_send()
        remote(st1.at[tp], st1.at[tp], st1_s.at[other], st1_r.at[tp], here).wait_send()
        remote(st2.at[tp], st2.at[tp], st2_s.at[other], st2_r.at[tp], here).wait_send()

    @pl.loop(0, EXPERTS)
    def _(e):
        @pl.when(jnp.logical_not(jnp.logical_and(own_self, e == sp)))
        def _():
            remote(send_rows.at[e], rb.at[0], disp_s.at[e], disp_r.at[0], here).wait_send()

        @pl.when(jnp.logical_not(jnp.logical_and(own_self, e == own_piece)))
        def _():
            remote(ob.at[0, 0, 0], rb.at[0], ret_s.at[e], ret_r.at[0], here).wait_send()

    for copy in xf + w_own + relays + [h_right, h_left, h_first, h_second]:
        copy.wait_send()


def body(
    pool_in,
    doc_ids,
    pool_map,
    pool_scale,
    w_out,
    gate_logit,
    residual,
    first_gain,
    first_bias,
    routes,
    route_weight,
    w_gate,
    w_up,
    w_down,
    second_gain,
    second_bias,
):
    vmem = pl.BlockSpec(memory_space=pltpu.VMEM)
    hbm = pl.BlockSpec(memory_space=pl.ANY)
    dma = pltpu.SemaphoreType.DMA
    args = (
        pool_in,
        doc_ids.reshape(1, -1),
        pool_map,
        pool_scale.reshape(1, -1),
        w_out,
        gate_logit,
        residual,
        first_gain.reshape(1, -1),
        first_bias.reshape(1, -1),
        routes,
        route_weight,
        w_gate[0],
        w_up[0],
        w_down[0],
        second_gain.reshape(1, -1),
        second_bias.reshape(1, -1),
    )
    in_specs = [vmem] * 11 + [hbm] * 3 + [vmem] * 2
    return pl.pallas_call(
        layer_kernel,
        out_shape=jax.ShapeDtypeStruct((TOK, FD), BF16),
        in_specs=in_specs,
        out_specs=vmem,
        scratch_shapes=[
            pltpu.VMEM((FEAT, HD), BF16),
            pltpu.VMEM((FEAT, HD), BF16),
            pltpu.VMEM((32, LANE), BF16),
            pltpu.VMEM((8, LANE), F32),
            pltpu.VMEM((BACK, 8, LANE), F32),
            pltpu.VMEM((NTP, 32, TOK), BF16),
            pltpu.VMEM((NTP, 2, TOK), F32),
            pltpu.VMEM((NTP, 2, TOK), F32),
            pltpu.VMEM((8, TOK), F32),
            pltpu.VMEM((EXPERTS, CAP, FD), BF16),
            pltpu.VMEM((NX, NG, NC, NY, CAP, FD), BF16),
            pltpu.VMEM((NY, FEAT, 2 * HD), BF16),
            pltpu.VMEM((NY, NTP * HD, FD), BF16),
            pltpu.VMEM((TOK, NY * LANE), F32),
            pltpu.VMEM((NX, TOK, NY * HD), BF16),
            pltpu.VMEM((NG, NC, NY, CAP, FD), BF16),
            pltpu.VMEM((EXPERTS, CAP, FD), BF16),
            pltpu.VMEM((2 * TOK, EXPERTS * CAP), BF16),
            pltpu.VMEM((TOK, FD), F32),
            dma((3,)),
            dma,
            dma,
            dma((BACK,)),
            dma((BACK,)),
            dma((NTP,)),
            dma((NTP,)),
            dma((NTP,)),
            dma((NTP,)),
            dma((NTP,)),
            dma((NTP,)),
            dma((EXPERTS,)),
            dma((PIECES,)),
            dma((3, NG)),
            dma((3, NG)),
            dma((8,)),
            dma((8,)),
            dma((4,)),
            dma((4,)),
            dma((PIECES,)),
            dma((EXPERTS,)),
        ],
        compiler_params=pltpu.CompilerParams(
            collective_id=0, has_side_effects=True, vmem_limit_bytes=48 * 1024 * 1024
        ),
        cost_estimate=pl.CostEstimate(
            flops=2_000_000_000, bytes_accessed=4_000_000, transcendentals=0
        ),
        name="layer",
    )(*args)


def solution(mesh):
    finer = Mesh(mesh.devices.reshape(NZ, NC, NY, NX), ("z", "core", "y", "x"))
    sp = ("z", "core")
    in_specs = (
        P(TP, sp),
        P(sp),
        P(),
        P(),
        P(None, TP),
        P(sp, TP),
        P(sp, TP),
        P(TP),
        P(TP),
        P(sp, None),
        P(sp, None),
        P(sp, None, TP),
        P(sp, None, TP),
        P(sp, None, TP),
        P(TP),
        P(TP),
    )
    return jax.shard_map(
        body, mesh=finer, in_specs=in_specs, out_specs=P(sp, TP), check_vma=False
    )
```

```python
import functools

import jax
import jax.numpy as jnp
from jax import lax
from jax.experimental import pallas as pl
from jax.experimental.pallas import tpu as pltpu
from jax.sharding import Mesh
from jax.sharding import PartitionSpec as P

MESH = pl.DeviceIdType.MESH
F32 = jnp.float32
BF16 = jnp.bfloat16
TP = ("y", "x")
EPS = 1e-05
ALPHA = 8.0**0.25
NZ, NC, NY, NX = 16, 2, 4, 4
NTP = NY * NX
EXPERTS = NZ * NC
CAP = 48
TOK = 384
MIX_W = 512
FEAT = 2048
FD = 128
HD = 64
LANE = 128
CHUNKS = TOK // LANE
BACK = 4
NG = NZ // NY
PIECES = NG * NC * NY
ORDER = (2, 1, 3, 0)


def dot(a, b, dims=((1,), (0,))):
    return lax.dot_general(a, b, (dims, ((), ())), preferred_element_type=F32)


def iota(shape, dim):
    return lax.broadcasted_iota(jnp.int32, shape, dim)


def turned(row):
    return jnp.broadcast_to(row, (LANE, LANE)).T


def part(value, k):
    return value[:, k * LANE : (k + 1) * LANE]


def rows_of(value, k):
    return value[k * LANE : (k + 1) * LANE]


def remote(src, dst, send, recv, where):
    return pltpu.make_async_remote_copy(
        src_ref=src, dst_ref=dst, send_sem=send, recv_sem=recv, device_id=where, device_id_type=MESH
    )


def norm_columns(totals):
    mean = totals[0:1] / FEAT
    var = totals[1:2] / FEAT - mean * mean
    return mean, lax.rsqrt(var + EPS)


def layer_kernel(
    pool_h,
    ids_h,
    pmap_h,
    scale_h,
    wout_h,
    gate_h,
    res_h,
    gain1_h,
    bias1_h,
    routes_h,
    rweight_h,
    wg_h,
    wu_h,
    wd_h,
    gain2_h,
    bias2_h,
    out_ref,
    pool_ref,
    ids_ref,
    pmap_ref,
    scale_ref,
    wout_ref,
    gate_ref,
    res_ref,
    gain1_ref,
    bias1_ref,
    routes_ref,
    rweight_ref,
    gain2_ref,
    bias2_ref,
    halo,
    pk,
    pk_in,
    pg,
    st1,
    st2,
    slots,
    send_rows,
    xb,
    wb,
    db,
    acc,
    hb,
    ob,
    rb,
    pick,
    nat,
    load_sem,
    near_sem,
    far_sem,
    halo_s,
    halo_r,
    pk_s,
    pk_r,
    pg_s,
    pg_r,
    st1_s,
    st1_r,
    st2_s,
    st2_r,
    disp_s,
    disp_r,
    xf_s,
    xf_r,
    w_s,
    w_r,
    h_s,
    h_r,
    ret_s,
    ret_r,
):
    z, c, y, x = (lax.axis_index(name) for name in ("z", "core", "y", "x"))
    here = (z, c, y, x)
    sp = z * NC + c
    tp = y * NX + x
    right, left = lax.rem(x + 1, NX), lax.rem(x + NX - 1, NX)
    across = lax.rem(x + 2, NX)
    down, up = lax.rem(y + 1, NY), lax.rem(y + NY - 1, NY)
    near = lax.rem(y - 2 * z + 2 * NZ, NY)
    own_self = near == 0
    own_place = c * NY + y

    def sp_device(k):
        return (k // NC, lax.rem(k, NC), y, x)

    def plane_device(k):
        return (z, c, k // NX, lax.rem(k, NX))

    def line_device(dz):
        return (lax.rem(z + dz + NZ, NZ), c, y, x)

    def expert_device(e):
        ze = e // NC
        return (ze, lax.rem(e, NC), lax.rem(z + ze, NY), x)

    def source_device(q, k):
        return (lax.rem(z + near + NY * q, NZ), k // NY, lax.rem(k, NY), x)

    def neighbour(yy):
        return (z, c, yy, x)

    def beside(xx):
        return (z, c, y, xx)

    def signal(sem, device):
        pl.semaphore_signal(sem, inc=1, device_id=device, device_id_type=MESH)

    loads = [
        pltpu.make_async_copy(src, dst, load_sem.at[k])
        for k, (src, dst) in enumerate(
            [
                (pool_h, pool_ref),
                (ids_h, ids_ref),
                (routes_h, routes_ref),
                (wg_h, wb.at[y, pl.ds(0, HD)]),
                (wu_h, wb.at[y, pl.ds(HD, HD)]),
                (wout_h, wout_ref),
                (gate_h, gate_ref),
                (res_h, res_ref),
                (pmap_h, pmap_ref),
                (scale_h, scale_ref),
                (gain1_h, gain1_ref),
                (bias1_h, bias1_ref),
                (wd_h, db.at[y]),
                (rweight_h, rweight_ref),
                (gain2_h, gain2_ref),
                (bias2_h, bias2_ref),
            ]
        )
    ]
    for load in loads:
        load.start()
    barrier = pltpu.get_barrier_semaphore()
    for dz in range(-2, 3):
        for other in range(NC):
            if dz:
                signal(barrier, (lax.rem(z + dz + NZ, NZ), other, y, x))
    signal(barrier, (z, 1 - c, y, x))

    @pl.loop(1, NTP)
    def _(k):
        signal(barrier, plane_device(lax.rem(tp + k, NTP)))

    loads[0].wait()
    loads[1].wait()
    ids = [ids_ref[k : k + 1, :].astype(F32) for k in range(CHUNKS)]
    pool = pool_ref[...]
    last_id = ids[CHUNKS - 1][:, LANE - 1 : LANE]
    tail = jnp.concatenate([(line == last_id).astype(F32) for line in ids], axis=1)
    tail = jnp.broadcast_to(tail, (8, TOK)).astype(BF16)
    padded = jnp.concatenate([pool, jnp.zeros((LANE - 32, TOK), BF16)], axis=0)
    padded = jnp.where(iota((LANE, TOK), 0) == 32, jnp.ones_like(padded), padded)
    sums = dot(tail, padded, ((1,), (1,)))
    line = iota((8, LANE), 0)
    packet = jnp.where(line == 0, sums, jnp.broadcast_to(last_id, (8, LANE)))
    packet = jnp.where(line == 2, jnp.broadcast_to(ids[CHUNKS - 1], (8, LANE)), packet)
    pk[...] = packet

    is_doc = x >= 2
    window = jnp.where(is_doc, 4 * TOK, jnp.left_shift(2, y))
    id_col = jnp.concatenate([turned(ids[k]) for k in range(CHUNKS)], axis=0)
    sum_own, count_own = [], []
    ones8 = jnp.ones((8, TOK), BF16)
    for k in range(CHUNKS):
        gap = iota((TOK, LANE), 1) + k * LANE - iota((TOK, LANE), 0)
        keep = (id_col == ids[k]) & (gap >= 0) & (gap < window)
        mask = keep.astype(F32).astype(BF16)
        sum_own.append(dot(pool, mask))
        count_own.append(dot(ones8, mask)[0:1])

    pl.semaphore_wait(barrier, NTP - 1 + 5 * NC - 1)

    for b in range(1, BACK + 1):

        @pl.when(sp + b < EXPERTS)
        def _():
            remote(
                pk, pk_in.at[b - 1], pk_s.at[b - 1], pk_r.at[b - 1], sp_device(sp + b)
            ).start()

    edge = pool_ref.at[:, pl.ds(TOK - LANE, LANE)]

    @pl.when(sp + 1 < EXPERTS)
    def _():
        remote(edge, halo, halo_s, halo_r, sp_device(sp + 1)).start()

    signal(near_sem, line_device(2))
    signal(near_sem, line_device(-2))

    weights = []

    def send_weights(source, first, count):
        k = 2 * len(weights)
        block = source.at[y, pl.ds(first, count)]
        pair = [
            remote(block, block, w_s.at[k], w_r.at[k], neighbour(down)),
            remote(block, block, w_s.at[k + 1], w_r.at[k + 1], neighbour(up)),
        ]
        for copy in pair:
            copy.start()
        weights.append(pair)

    loads[3].wait()
    loads[4].wait()
    send_weights(wb, 0, 32)

    for k in (2, *range(5, len(loads))):
        loads[k].wait()
    wout_t = jnp.concatenate(
        [rows_of(wout_ref[...], k).astype(F32).T for k in range(MIX_W // LANE)], axis=1
    ).astype(BF16)
    gate_t = jnp.concatenate(
        [rows_of(gate_ref[...], k).astype(F32).T for k in range(CHUNKS)], axis=1
    )
    gate_t = jax.nn.sigmoid(gate_t)
    res_t = ALPHA * jnp.concatenate(
        [rows_of(res_ref[...], k).astype(F32).T for k in range(CHUNKS)], axis=1
    )
    none = jnp.zeros((HD, HD), F32)
    maps = []
    for k in range(MIX_W // LANE):
        upper = jnp.concatenate([pmap_ref[2 * k].astype(F32), none], axis=1)
        lower = jnp.concatenate([none, pmap_ref[2 * k + 1].astype(F32)], axis=1)
        maps.append(jnp.concatenate([upper, lower], axis=0).T.astype(BF16))
    scales = [turned(part(scale_ref[...], k)) for k in range(MIX_W // LANE)]
    gain1 = turned(gain1_ref[...])
    bias1 = turned(bias1_ref[...])

    @pl.when(sp >= 1)
    def _():
        remote(edge, halo, halo_s, halo_r, here).wait_recv()

    for b in range(1, BACK + 1):

        @pl.when(sp >= b)
        def _():
            remote(pk, pk_in.at[b - 1], pk_s.at[b - 1], pk_r.at[b - 1], here).wait_recv()

    first_id = jnp.broadcast_to(ids[0][:, 0:1], (1, LANE))
    carry = jnp.zeros((1, LANE), F32)
    for b in range(1, BACK + 1):
        found = pk_in[b - 1]
        same = (found[1:2] == first_id) & (jnp.broadcast_to(sp, (1, LANE)) >= b)
        carry = carry + jnp.where(same, found[0:1], 0.0)
    carry_col = turned(carry)
    doc_flag = is_doc.astype(F32)
    halo_on = jnp.broadcast_to(jnp.logical_and(sp >= 1, x < 2), (LANE, LANE))
    halo_ids = turned(pk_in[0][2:3])
    gap = iota((LANE, LANE), 1) + LANE - iota((LANE, LANE), 0)
    keep = (halo_ids == ids[0]) & (gap < window) & halo_on
    mask = keep.astype(F32).astype(BF16)
    halo_in = jnp.where(halo_on[0:32], halo[...].astype(F32), 0.0).astype(BF16)
    halo_sum = dot(halo_in, mask)
    halo_count = dot(ones8[:, :LANE], mask)[0:1]
    for k in range(CHUNKS):
        head = (ids[k] == first_id).astype(F32) * doc_flag
        total = sum_own[k] + carry_col[0:32] * head
        count = count_own[k] + carry_col[32:33] * head
        if k == 0:
            total = total + halo_sum
            count = count + halo_count
        pooled = total / count - part(pool, k).astype(F32)
        pg[tp, :, k * LANE : (k + 1) * LANE] = pooled.astype(BF16)

    @pl.loop(1, NTP)
    def _(k):
        other = lax.rem(tp + k, NTP)
        remote(pg.at[tp], pg.at[tp], pg_s.at[other], pg_r.at[tp], plane_device(other)).start()

    send_weights(wb, 32, 16)
    pl.semaphore_wait(near_sem, 2)
    signal(far_sem, line_device(4))
    signal(far_sem, line_device(-4))

    expert = iota((EXPERTS, TOK), 0).astype(F32)
    ways = [(expert == routes_ref[k : k + 1, :].astype(F32)).astype(F32) for k in range(2)]
    earlier = (iota((TOK, TOK), 0) < iota((TOK, TOK), 1)).astype(F32).astype(BF16)
    rank = dot((ways[0] + ways[1]).astype(BF16), earlier) + expert * CAP
    for k in range(2):
        slots[k : k + 1, :] = jnp.sum(ways[k] * rank, axis=0, keepdims=True)

    @pl.loop(1, NTP)
    def _(k):
        other = lax.rem(tp + k, NTP)
        remote(pg.at[tp], pg.at[other], pg_s.at[other], pg_r.at[other], here).wait_recv()

    mapped = []
    for k in range(MIX_W // LANE):
        grouped = dot(maps[k], pg[4 * k : 4 * k + 4].reshape(LANE, TOK))
        scaled = [part(grouped, j) * scales[k] for j in range(CHUNKS)]
        mapped.append(jnp.concatenate(scaled, axis=1).astype(BF16))
    mixed = res_t + dot(wout_t, jnp.concatenate(mapped, axis=0)) * gate_t
    st1[tp, 0:1] = jnp.sum(mixed, axis=0, keepdims=True)
    st1[tp, 1:2] = jnp.sum(mixed * mixed, axis=0, keepdims=True)

    pl.semaphore_wait(far_sem, 2)

    @pl.loop(1, NTP)
    def _(k):
        other = lax.rem(tp + k, NTP)
        remote(st1.at[tp], st1.at[tp], st1_s.at[other], st1_r.at[tp], plane_device(other)).start()

    send_weights(wb, 48, 64)

    @pl.loop(1, NTP)
    def _(k):
        other = lax.rem(tp + k, NTP)
        remote(st1.at[tp], st1.at[other], st1_s.at[other], st1_r.at[other], here).wait_recv()

    mean, rstd = norm_columns(jnp.sum(st1[...], axis=0))
    centred = (mixed - mean) * rstd
    normed = jnp.concatenate(
        [part(centred, k) * gain1 + bias1 for k in range(CHUNKS)], axis=1
    ).astype(BF16)

    for k in range(8):
        first = k * (EXPERTS * CAP // 8)
        place = (iota((EXPERTS * CAP // 8, TOK), 0) + first).astype(F32)
        chosen = (place == slots[0:1, :]) | (place == slots[1:2, :])
        rows = dot(chosen.astype(F32).astype(BF16), normed, ((1,), (1,)))
        send_rows[4 * k : 4 * k + 4] = rows.astype(BF16).reshape(4, CAP, FD)

    for q in ORDER:

        @pl.loop(0, NY * NC)
        def _(k):
            ze = lax.rem(z - k // NC - NY * q + 2 * NZ, NZ)
            e = ze * NC + lax.rem(k, NC)

            @pl.when(jnp.logical_not(jnp.logical_and(own_self, e == sp)))
            def _():
                remote(
                    send_rows.at[e],
                    xb.at[x, q, c, y],
                    disp_s.at[e],
                    disp_r.at[q, own_place],
                    expert_device(e),
                ).start()

    @pl.when(own_self)
    def _():
        xb[x, 0, c, y] = send_rows[sp]

    send_weights(wb, 112, 16)
    send_weights(db, 0, NTP * HD)

    for k in range(CHUNKS):
        nat[k * LANE : (k + 1) * LANE] = part(normed, k).astype(F32).T
        for way in range(2):
            column = turned(slots[way : way + 1, k * LANE : (k + 1) * LANE])
            for j in range(EXPERTS * CAP // LANE):
                lane = (iota((LANE, LANE), 1) + j * LANE).astype(F32)
                pick[way * TOK + k * LANE : way * TOK + (k + 1) * LANE, j * LANE : (j + 1) * LANE] = (
                    (lane == column).astype(F32).astype(BF16)
                )

    relays = []

    def relay_weights(source, count):
        k = 2 * len(weights) + len(relays)
        from_up = source.at[up, pl.ds(0, count)]
        from_down = source.at[down, pl.ds(count, count)]
        pair = [
            remote(from_up, from_up, w_s.at[k], w_r.at[k], neighbour(down)),
            remote(from_down, from_down, w_s.at[k + 1], w_r.at[k + 1], neighbour(up)),
        ]
        for copy in pair:
            copy.start()
        relays.extend(pair)

    def wait_weights(first, last):
        for pair in weights[first:last]:
            for copy in pair:
                copy.wait_recv()

    xf, xr = {}, {}

    def arrive(q):
        @pl.loop(0, NC * NY)
        def _(k):
            mine = jnp.logical_and(own_self, k == own_place) if q == 0 else jnp.bool_(False)

            @pl.when(jnp.logical_not(mine))
            def _():
                remote(
                    send_rows.at[0],
                    xb.at[x, q, k // NY, lax.rem(k, NY)],
                    disp_s.at[0],
                    disp_r.at[q, k],
                    here,
                ).wait_recv()

        mine = xb.at[x, q]
        xf[q] = [
            remote(mine, mine, xf_s.at[0, q], xf_r.at[0, q], beside(right)),
            remote(mine, mine, xf_s.at[1, q], xf_r.at[1, q], beside(left)),
        ]
        for copy in xf[q]:
            copy.start()

    def relay_rows(q, to_right):
        for copy in xf[q]:
            copy.wait_recv()
        piece = xb.at[left if to_right else right, q]
        xr[q] = remote(
            piece, piece, xf_s.at[2, q], xf_r.at[2, q], beside(right if to_right else left)
        )
        xr[q].start()

    def projected(pair, xx):
        tiles, columns = [], []
        for yy in range(NY):
            block = [xb[xx, q, :, yy].reshape(NC * CAP, FD) for q in pair]
            tiles.append(jnp.concatenate(block, axis=0))
            start = pl.multiple_of((yy * NX + xx) * FD, FD)
            columns.append(
                jnp.concatenate([wb[b, :, pl.ds(start, FD)] for b in range(NY)], axis=0)
            )
        return dot(
            jnp.concatenate(tiles, axis=1), jnp.concatenate(columns, axis=1), ((1,), (1,))
        )

    half = TOK // 2
    low = iota((half, LANE), 1) < HD

    def hidden_rows(number, pair):
        for q in pair:
            xr[q].wait_recv()
        acc[...] = projected(pair, x)
        for xx in (left, right, across):
            acc[...] += projected(pair, xx)
        for k in range(NY // 2):
            one = acc[:, 2 * k * LANE : (2 * k + 1) * LANE]
            two = acc[:, (2 * k + 1) * LANE : (2 * k + 2) * LANE]
            gate = jnp.where(low, one, pltpu.roll(two, HD, 1))
            lift = jnp.where(low, pltpu.roll(one, HD, 1), two)
            hidden = gate * jax.nn.sigmoid(gate) * lift
            hb[x, number, :, k * LANE : (k + 1) * LANE] = hidden.astype(BF16)
        mine = hb.at[x, number]
        copies = [
            remote(mine, mine, h_s.at[number, 0], h_r.at[number, 0], beside(right)),
            remote(mine, mine, h_s.at[number, 1], h_r.at[number, 1], beside(left)),
        ]
        for copy in copies:
            copy.start()
        return copies

    def relay_hidden(number, copies):
        copies[0].wait_recv()
        piece = hb.at[left, number, pl.ds(0, half // 2)]
        first = remote(piece, piece, h_s.at[number, 2], h_r.at[number, 2], beside(right))
        first.start()
        copies[1].wait_recv()
        piece = hb.at[right, number, pl.ds(half // 2, half // 2)]
        second = remote(piece, piece, h_s.at[number, 3], h_r.at[number, 3], beside(left))
        second.start()
        copies += [first, second]

    def lowered(number, xx):
        blocks = []
        for yy in range(NY):
            pieces = [
                db[yy, pl.ds(pl.multiple_of((b * NX + xx) * HD, HD), HD), :] for b in range(NY)
            ]
            blocks.append(jnp.concatenate(pieces, axis=0))
        return dot(hb[xx, number], jnp.concatenate(blocks, axis=1))

    def give_back(number, pair, copies):
        acc[...] = lowered(number, x)
        acc[...] += lowered(number, left)
        acc[...] += lowered(number, right)
        copies[2].wait_recv()
        copies[3].wait_recv()
        result = (acc[...] + lowered(number, across)).astype(BF16)
        for k, q in enumerate(pair):
            rows = result[k * NC * CAP : (k + 1) * NC * CAP]
            for yy in range(NY):
                ob[q, :, yy] = part(rows, yy).reshape(NC, CAP, FD)

            @pl.loop(0, NC * NY)
            def _(k):
                mine = jnp.logical_and(own_self, k == own_place) if q == 0 else jnp.bool_(False)

                @pl.when(jnp.logical_not(mine))
                def _():
                    remote(
                        ob.at[q, k // NY, lax.rem(k, NY)],
                        rb.at[sp],
                        ret_s.at[q, k],
                        ret_r.at[sp],
                        source_device(q, k),
                    ).start()

    far_half, near_half = ORDER[:2], ORDER[2:]
    arrive(far_half[0])
    arrive(far_half[1])
    wait_weights(0, 4)
    relay_weights(wb, HD)
    relay_rows(far_half[0], True)
    arrive(near_half[0])
    relay_rows(far_half[1], False)
    arrive(near_half[1])
    for copy in relays[:2]:
        copy.wait_recv()
    hidden_far = hidden_rows(0, far_half)
    relay_rows(near_half[0], True)
    relay_rows(near_half[1], False)
    wait_weights(4, 5)
    relay_weights(db, NTP * HD // 2)
    relay_hidden(0, hidden_far)
    hidden_near = hidden_rows(1, near_half)
    for copy in relays[2:]:
        copy.wait_recv()
    give_back(0, far_half, hidden_far)
    relay_hidden(1, hidden_near)
    give_back(1, near_half, hidden_near)

    @pl.when(own_self)
    def _():
        rb[sp] = ob[0, c, y]

    for b in range(1, BACK + 1):

        @pl.when(sp + b < EXPERTS)
        def _():
            remote(pk, pk_in.at[b - 1], pk_s.at[b - 1], pk_r.at[b - 1], here).wait_send()

    @pl.when(sp + 1 < EXPERTS)
    def _():
        remote(edge, halo, halo_s, halo_r, here).wait_send()

    @pl.loop(1, NTP)
    def _(k):
        other = lax.rem(tp + k, NTP)
        remote(pg.at[tp], pg.at[tp], pg_s.at[other], pg_r.at[tp], here).wait_send()
        remote(st1.at[tp], st1.at[tp], st1_s.at[other], st1_r.at[tp], here).wait_send()

    @pl.loop(0, EXPERTS)
    def _(e):
        @pl.when(jnp.logical_not(jnp.logical_and(own_self, e == sp)))
        def _():
            remote(send_rows.at[e], rb.at[0], disp_s.at[e], disp_r.at[0, 0], here).wait_send()

    for pair in weights:
        relays.extend(pair)
    for copies in list(xf.values()) + [list(xr.values()), relays, hidden_far, hidden_near]:
        for copy in copies:
            copy.wait_send()

    @pl.loop(0, EXPERTS)
    def _(e):
        @pl.when(jnp.logical_not(jnp.logical_and(own_self, e == sp)))
        def _():
            remote(ob.at[0, 0, 0], rb.at[e], ret_s.at[0, 0], ret_r.at[e], here).wait_recv()

    picked = dot(pick[...], rb[...].reshape(EXPERTS * CAP, FD))
    moe = []
    for k in range(CHUNKS):
        both = [turned(rweight_ref[way : way + 1, k * LANE : (k + 1) * LANE]) for way in range(2)]
        moe.append(
            rows_of(picked, k) * both[0] + rows_of(picked, CHUNKS + k) * both[1]
        )
    final = ALPHA * nat[...] + jnp.concatenate(moe, axis=0)
    for k in range(CHUNKS):
        block = rows_of(final, k).T
        st2[tp, 0:1, k * LANE : (k + 1) * LANE] = jnp.sum(block, axis=0, keepdims=True)
        st2[tp, 1:2, k * LANE : (k + 1) * LANE] = jnp.sum(block * block, axis=0, keepdims=True)

    @pl.loop(1, NTP)
    def _(k):
        other = lax.rem(tp + k, NTP)
        remote(st2.at[tp], st2.at[tp], st2_s.at[other], st2_r.at[tp], plane_device(other)).start()

    @pl.loop(0, PIECES)
    def _(k):
        @pl.when(jnp.logical_not(jnp.logical_and(own_self, k == own_place)))
        def _():
            remote(
                ob.at[0, 0, 0],
                rb.at[0],
                ret_s.at[k // (NC * NY), lax.rem(k, NC * NY)],
                ret_r.at[0],
                here,
            ).wait_send()

    @pl.loop(1, NTP)
    def _(k):
        other = lax.rem(tp + k, NTP)
        remote(st2.at[tp], st2.at[other], st2_s.at[other], st2_r.at[other], here).wait_recv()

    mean, rstd = norm_columns(jnp.sum(st2[...], axis=0))
    for k in range(CHUNKS):
        centred = (rows_of(final, k) - turned(part(mean, k))) * turned(part(rstd, k))
        out_ref[k * LANE : (k + 1) * LANE, :] = (
            centred * gain2_ref[...] + bias2_ref[...]
        ).astype(BF16)

    @pl.loop(1, NTP)
    def _(k):
        other = lax.rem(tp + k, NTP)
        remote(st2.at[tp], st2.at[tp], st2_s.at[other], st2_r.at[tp], here).wait_send()


def body(
    pool_in,
    doc_ids,
    pool_map,
    pool_scale,
    w_out,
    gate_logit,
    residual,
    first_gain,
    first_bias,
    routes,
    route_weight,
    w_gate,
    w_up,
    w_down,
    second_gain,
    second_bias,
):
    vmem = pl.BlockSpec(memory_space=pltpu.VMEM)
    hbm = pl.BlockSpec(memory_space=pltpu.HBM)
    dma = pltpu.SemaphoreType.DMA
    args = (
        pool_in,
        doc_ids.reshape(CHUNKS, LANE),
        pool_map,
        pool_scale.reshape(1, -1),
        w_out,
        gate_logit,
        residual,
        first_gain.reshape(1, -1),
        first_bias.reshape(1, -1),
        routes.T,
        route_weight.T,
        w_gate[0].T,
        w_up[0].T,
        w_down[0],
        second_gain.reshape(1, -1),
        second_bias.reshape(1, -1),
    )
    in_specs = [hbm] * len(args)
    return pl.pallas_call(
        layer_kernel,
        out_shape=jax.ShapeDtypeStruct((TOK, FD), BF16),
        in_specs=in_specs,
        out_specs=vmem,
        scratch_shapes=[
            pltpu.VMEM((32, TOK), BF16),
            pltpu.VMEM((CHUNKS, LANE), jnp.int32),
            pltpu.VMEM((2 * NG, HD, HD), BF16),
            pltpu.VMEM((1, MIX_W), F32),
            pltpu.VMEM((MIX_W, FD), BF16),
            pltpu.VMEM((TOK, FD), BF16),
            pltpu.VMEM((TOK, FD), BF16),
            pltpu.VMEM((1, FD), F32),
            pltpu.VMEM((1, FD), F32),
            pltpu.VMEM((2, TOK), jnp.int32),
            pltpu.VMEM((2, TOK), F32),
            pltpu.VMEM((1, FD), F32),
            pltpu.VMEM((1, FD), F32),
            pltpu.VMEM((32, LANE), BF16),
            pltpu.VMEM((8, LANE), F32),
            pltpu.VMEM((BACK, 8, LANE), F32),
            pltpu.VMEM((NTP, 32, TOK), BF16),
            pltpu.VMEM((NTP, 2, TOK), F32),
            pltpu.VMEM((NTP, 2, TOK), F32),
            pltpu.VMEM((2, TOK), F32),
            pltpu.VMEM((EXPERTS, CAP, FD), BF16),
            pltpu.VMEM((NX, NG, NC, NY, CAP, FD), BF16),
            pltpu.VMEM((NY, 2 * HD, FEAT), BF16),
            pltpu.VMEM((NY, NTP * HD, FD), BF16),
            pltpu.VMEM((TOK // 2, NY * LANE), F32),
            pltpu.VMEM((NX, 2, TOK // 2, NY * HD), BF16),
            pltpu.VMEM((NG, NC, NY, CAP, FD), BF16),
            pltpu.VMEM((EXPERTS, CAP, FD), BF16),
            pltpu.VMEM((2 * TOK, EXPERTS * CAP), BF16),
            pltpu.VMEM((TOK, FD), F32),
            dma((len(args),)),
            pltpu.SemaphoreType.REGULAR,
            pltpu.SemaphoreType.REGULAR,
            dma,
            dma,
            dma((BACK,)),
            dma((BACK,)),
            dma((NTP,)),
            dma((NTP,)),
            dma((NTP,)),
            dma((NTP,)),
            dma((NTP,)),
            dma((NTP,)),
            dma((EXPERTS,)),
            dma((NG, NC * NY)),
            dma((3, NG)),
            dma((3, NG)),
            dma((16,)),
            dma((16,)),
            dma((2, 4)),
            dma((2, 4)),
            dma((NG, NC * NY)),
            dma((EXPERTS,)),
        ],
        compiler_params=pltpu.CompilerParams(
            collective_id=0, has_side_effects=True, vmem_limit_bytes=66_000_000
        ),
        cost_estimate=pl.CostEstimate(
            flops=2_000_000_000, bytes_accessed=4_000_000, transcendentals=0
        ),
        name="layer",
    )(*args)


def solution(mesh):
    finer = Mesh(mesh.devices.reshape(NZ, NC, NY, NX), ("z", "core", "y", "x"))
    sp = ("z", "core")
    in_specs = (
        P(TP, sp),
        P(sp),
        P(),
        P(),
        P(None, TP),
        P(sp, TP),
        P(sp, TP),
        P(TP),
        P(TP),
        P(sp, None),
        P(sp, None),
        P(sp, None, TP),
        P(sp, None, TP),
        P(sp, None, TP),
        P(TP),
        P(TP),
    )
    return jax.shard_map(
        body, mesh=finer, in_specs=in_specs, out_specs=P(sp, TP), check_vma=False
    )
```

```python
import functools

import jax
import jax.numpy as jnp
from jax import lax
from jax.experimental import pallas as pl
from jax.experimental.pallas import tpu as pltpu
from jax.sharding import Mesh
from jax.sharding import PartitionSpec as P

MESH = pl.DeviceIdType.MESH
F32 = jnp.float32
BF16 = jnp.bfloat16
TP = ("y", "x")
EPS = 1e-05
ALPHA = 8.0**0.25
NZ, NC, NY, NX = 16, 2, 4, 4
NTP = NY * NX
EXPERTS = NZ * NC
CAP = 48
TOK = 384
MIX_W = 512
FEAT = 2048
FD = 128
HD = 64
LANE = 128
CHUNKS = TOK // LANE
BACK = 4
NG = NZ // NY
PIECES = NG * NC * NY
ORDER = (2, 1, 3, 0)
GROUP = NC * CAP
STEPS = ("a2", "a1", "g2", "a3", "g1", "a0", "d2", "g3", "d1", "g0", "d3", "d0")
HOPS = sorted(
    ((dy, dx) for dy in range(NY) for dx in range(NX) if dy or dx),
    key=lambda d: -min(d[0], NY - d[0]) - min(d[1], NX - d[1]),
)


def dot(a, b, dims=((1,), (0,))):
    return lax.dot_general(a, b, (dims, ((), ())), preferred_element_type=F32)


def iota(shape, dim):
    return lax.broadcasted_iota(jnp.int32, shape, dim)


def turned(row):
    return jnp.broadcast_to(row, (LANE, LANE)).T


def part(value, k):
    return value[:, k * LANE : (k + 1) * LANE]


def rows_of(value, k):
    return value[k * LANE : (k + 1) * LANE]


def remote(src, dst, send, recv, where):
    return pltpu.make_async_remote_copy(
        src_ref=src, dst_ref=dst, send_sem=send, recv_sem=recv, device_id=where, device_id_type=MESH
    )


def norm_columns(totals):
    mean = totals[0:1] / FEAT
    var = totals[1:2] / FEAT - mean * mean
    return mean, lax.rsqrt(var + EPS)


def layer_kernel(
    pool_h,
    ids_h,
    pmap_h,
    scale_h,
    wout_h,
    gate_h,
    res_h,
    gain1_h,
    bias1_h,
    routes_h,
    rweight_h,
    wg_h,
    wu_h,
    wd_h,
    gain2_h,
    bias2_h,
    out_ref,
    pool_ref,
    ids_ref,
    pmap_ref,
    scale_ref,
    wout_ref,
    gate_ref,
    res_ref,
    gain1_ref,
    bias1_ref,
    routes_ref,
    rweight_ref,
    gain2_ref,
    bias2_ref,
    halo,
    pk,
    pk_in,
    pg,
    st1,
    st2,
    slots,
    send_rows,
    xb,
    wb,
    db,
    acc,
    hb,
    ob,
    rb,
    pick,
    nat,
    load_sem,
    near_sem,
    far_sem,
    halo_s,
    halo_r,
    pk_s,
    pk_r,
    pg_s,
    pg_r,
    st1_s,
    st1_r,
    st2_s,
    st2_r,
    disp_s,
    disp_r,
    xf_s,
    xf_r,
    w_s,
    w_r,
    h_s,
    h_r,
    ret_s,
    ret_r,
):
    z, c, y, x = (lax.axis_index(name) for name in ("z", "core", "y", "x"))
    here = (z, c, y, x)
    sp = z * NC + c
    tp = y * NX + x
    a = jnp.where(c == 0, y, x)
    b = jnp.where(c == 0, x, y)
    a_step = jnp.where(c == 0, NX, 1)
    b_step = jnp.where(c == 0, 1, NX)
    right, left = lax.rem(b + 1, NX), lax.rem(b + NX - 1, NX)
    across = lax.rem(b + 2, NX)
    down, up = lax.rem(a + 1, NY), lax.rem(a + NY - 1, NY)
    near = lax.rem(a - 2 * z + 2 * NZ, NY)
    own_self = near == 0
    own_place = c * NY + a

    def sp_device(k):
        return (k // NC, lax.rem(k, NC), y, x)

    def plane_device(k):
        return (z, c, k // NX, lax.rem(k, NX))

    def to_plane(buffer, send, recv):
        for dy, dx in HOPS:
            yy, xx = lax.rem(y + dy, NY), lax.rem(x + dx, NX)
            other = yy * NX + xx
            remote(
                buffer.at[tp], buffer.at[tp], send.at[other], recv.at[tp], (z, c, yy, xx)
            ).start()

    def line_device(dz):
        return (lax.rem(z + dz + NZ, NZ), c, y, x)

    def turned_device(zz, cc, aa, bb):
        first = cc == 0
        return (zz, cc, jnp.where(first, aa, bb), jnp.where(first, bb, aa))

    def expert_device(r):
        ze = (z - r // NC) & (NZ - 1)
        row = (z + ze) & (NY - 1)
        return (ze, 0, row, x) if r % NC == 0 else (ze, 1, y, row)

    def unless(mine, act):
        if mine is None:
            act()
        else:
            pl.when(jnp.logical_not(mine))(lambda: act())

    def is_mine(q, k):
        return jnp.logical_and(own_self, own_place == k) if q == 0 else None

    def source_device(q, k):
        other = k % NY
        return (
            (z + near + NY * q) & (NZ - 1),
            k // NY,
            jnp.where(c == 0, other, b),
            jnp.where(c == 0, b, other),
        )

    def neighbour(aa):
        return turned_device(z, c, aa, b)

    def beside(bb):
        return turned_device(z, c, a, bb)

    def signal(sem, device):
        pl.semaphore_signal(sem, inc=1, device_id=device, device_id_type=MESH)

    loads = [
        pltpu.make_async_copy(src, dst, load_sem.at[k])
        for k, (src, dst) in enumerate(
            [
                (pool_h, pool_ref),
                (ids_h, ids_ref),
                (routes_h, routes_ref),
                (wg_h, wb.at[a, pl.ds(0, HD)]),
                (wu_h, wb.at[a, pl.ds(HD, HD)]),
                (wout_h, wout_ref),
                (gate_h, gate_ref),
                (res_h, res_ref),
                (pmap_h, pmap_ref),
                (scale_h, scale_ref),
                (gain1_h, gain1_ref),
                (bias1_h, bias1_ref),
                (wd_h, db.at[a]),
                (rweight_h, rweight_ref),
                (gain2_h, gain2_ref),
                (bias2_h, bias2_ref),
            ]
        )
    ]
    for load in loads:
        load.start()
    barrier = pltpu.get_barrier_semaphore()
    for dz in range(-2, 3):
        for other in range(NC):
            if dz:
                signal(barrier, (lax.rem(z + dz + NZ, NZ), other, y, x))
    signal(barrier, (z, 1 - c, y, x))

    @pl.loop(1, NTP)
    def _(k):
        signal(barrier, plane_device(lax.rem(tp + k, NTP)))

    loads[0].wait()
    loads[1].wait()
    ids = [ids_ref[k : k + 1, :].astype(F32) for k in range(CHUNKS)]
    pool = pool_ref[...]
    last_id = ids[CHUNKS - 1][:, LANE - 1 : LANE]
    tail = jnp.concatenate([(line == last_id).astype(F32) for line in ids], axis=1)
    tail = jnp.broadcast_to(tail, (8, TOK)).astype(BF16)
    padded = jnp.concatenate([pool, jnp.zeros((LANE - 32, TOK), BF16)], axis=0)
    padded = jnp.where(iota((LANE, TOK), 0) == 32, jnp.ones_like(padded), padded)
    sums = dot(tail, padded, ((1,), (1,)))
    line = iota((8, LANE), 0)
    packet = jnp.where(line == 0, sums, jnp.broadcast_to(last_id, (8, LANE)))
    packet = jnp.where(line == 2, jnp.broadcast_to(ids[CHUNKS - 1], (8, LANE)), packet)
    pk[...] = packet

    is_doc = x >= 2
    window = jnp.where(is_doc, 4 * TOK, jnp.left_shift(2, y))
    id_col = jnp.concatenate([turned(ids[k]) for k in range(CHUNKS)], axis=0)
    sum_own, count_own = [], []
    ones8 = jnp.ones((8, TOK), BF16)
    for k in range(CHUNKS):
        gap = iota((TOK, LANE), 1) + k * LANE - iota((TOK, LANE), 0)
        keep = (id_col == ids[k]) & (gap >= 0) & (gap < window)
        mask = keep.astype(F32).astype(BF16)
        sum_own.append(dot(pool, mask))
        count_own.append(dot(ones8, mask)[0:1])

    pl.semaphore_wait(barrier, NTP - 1 + 5 * NC - 1)

    for back in range(1, BACK + 1):

        @pl.when(sp + back < EXPERTS)
        def _():
            remote(
                pk,
                pk_in.at[back - 1],
                pk_s.at[back - 1],
                pk_r.at[back - 1],
                sp_device(sp + back),
            ).start()

    edge = pool_ref.at[:, pl.ds(TOK - LANE, LANE)]

    @pl.when(sp + 1 < EXPERTS)
    def _():
        remote(edge, halo, halo_s, halo_r, sp_device(sp + 1)).start()

    signal(near_sem, line_device(2))
    signal(near_sem, line_device(-2))

    weights = []

    def send_weights(source, first, count):
        k = 2 * len(weights)
        block = source.at[a, pl.ds(first, count)]
        pair = [
            remote(block, block, w_s.at[k], w_r.at[k], neighbour(down)),
            remote(block, block, w_s.at[k + 1], w_r.at[k + 1], neighbour(up)),
        ]
        for copy in pair:
            copy.start()
        weights.append(pair)

    loads[3].wait()
    loads[4].wait()
    send_weights(wb, 0, 64)

    for k in (2, *range(5, len(loads))):
        loads[k].wait()
    wout_t = jnp.concatenate(
        [rows_of(wout_ref[...], k).astype(F32).T for k in range(MIX_W // LANE)], axis=1
    ).astype(BF16)
    gate_t = jnp.concatenate(
        [rows_of(gate_ref[...], k).astype(F32).T for k in range(CHUNKS)], axis=1
    )
    gate_t = jax.nn.sigmoid(gate_t)
    res_t = ALPHA * jnp.concatenate(
        [rows_of(res_ref[...], k).astype(F32).T for k in range(CHUNKS)], axis=1
    )
    none = jnp.zeros((HD, HD), F32)
    maps = []
    for k in range(MIX_W // LANE):
        upper = jnp.concatenate([pmap_ref[2 * k].astype(F32), none], axis=1)
        lower = jnp.concatenate([none, pmap_ref[2 * k + 1].astype(F32)], axis=1)
        maps.append(jnp.concatenate([upper, lower], axis=0).T.astype(BF16))
    scales = [turned(part(scale_ref[...], k)) for k in range(MIX_W // LANE)]
    gain1 = turned(gain1_ref[...])
    bias1 = turned(bias1_ref[...])

    @pl.when(sp >= 1)
    def _():
        remote(edge, halo, halo_s, halo_r, here).wait_recv()

    for back in range(1, BACK + 1):

        @pl.when(sp >= back)
        def _():
            remote(
                pk, pk_in.at[back - 1], pk_s.at[back - 1], pk_r.at[back - 1], here
            ).wait_recv()

    first_id = jnp.broadcast_to(ids[0][:, 0:1], (1, LANE))
    carry = jnp.zeros((1, LANE), F32)
    for back in range(1, BACK + 1):
        found = pk_in[back - 1]
        same = (found[1:2] == first_id) & (jnp.broadcast_to(sp, (1, LANE)) >= back)
        carry = carry + jnp.where(same, found[0:1], 0.0)
    carry_col = turned(carry)
    doc_flag = is_doc.astype(F32)
    halo_on = jnp.broadcast_to(jnp.logical_and(sp >= 1, x < 2), (LANE, LANE))
    halo_ids = turned(pk_in[0][2:3])
    gap = iota((LANE, LANE), 1) + LANE - iota((LANE, LANE), 0)
    keep = (halo_ids == ids[0]) & (gap < window) & halo_on
    mask = keep.astype(F32).astype(BF16)
    halo_in = jnp.where(halo_on[0:32], halo[...].astype(F32), 0.0).astype(BF16)
    halo_sum = dot(halo_in, mask)
    halo_count = dot(ones8[:, :LANE], mask)[0:1]
    for k in range(CHUNKS):
        head = (ids[k] == first_id).astype(F32) * doc_flag
        total = sum_own[k] + carry_col[0:32] * head
        count = count_own[k] + carry_col[32:33] * head
        if k == 0:
            total = total + halo_sum
            count = count + halo_count
        pooled = total / count - part(pool, k).astype(F32)
        pg[tp, :, k * LANE : (k + 1) * LANE] = pooled.astype(BF16)

    to_plane(pg, pg_s, pg_r)

    send_weights(wb, 64, 16)
    pl.semaphore_wait(near_sem, 2)
    signal(far_sem, line_device(4))
    signal(far_sem, line_device(-4))

    expert = iota((EXPERTS, TOK), 0).astype(F32)
    routes = routes_ref[...]
    routes = ((z - routes // NC) & (NZ - 1)) * NC + (routes & (NC - 1))
    ways = [(expert == routes[k : k + 1].astype(F32)).astype(F32) for k in range(2)]
    earlier = (iota((TOK, TOK), 0) < iota((TOK, TOK), 1)).astype(F32).astype(BF16)
    rank = dot((ways[0] + ways[1]).astype(BF16), earlier) + expert * CAP
    for k in range(2):
        slots[k : k + 1, :] = jnp.sum(ways[k] * rank, axis=0, keepdims=True)

    @pl.loop(1, NTP)
    def _(k):
        other = lax.rem(tp + k, NTP)
        remote(pg.at[tp], pg.at[other], pg_s.at[other], pg_r.at[other], here).wait_recv()

    mapped = []
    for k in range(MIX_W // LANE):
        grouped = dot(maps[k], pg[4 * k : 4 * k + 4].reshape(LANE, TOK))
        scaled = [part(grouped, j) * scales[k] for j in range(CHUNKS)]
        mapped.append(jnp.concatenate(scaled, axis=1).astype(BF16))
    mixed = res_t + dot(wout_t, jnp.concatenate(mapped, axis=0)) * gate_t
    st1[tp, 0:1] = jnp.sum(mixed, axis=0, keepdims=True)
    st1[tp, 1:2] = jnp.sum(mixed * mixed, axis=0, keepdims=True)

    pl.semaphore_wait(far_sem, 2)

    to_plane(st1, st1_s, st1_r)

    send_weights(wb, 80, 48)
    send_weights(db, 0, NTP * HD)

    @pl.loop(1, NTP)
    def _(k):
        other = lax.rem(tp + k, NTP)
        remote(st1.at[tp], st1.at[other], st1_s.at[other], st1_r.at[other], here).wait_recv()

    mean, rstd = norm_columns(jnp.sum(st1[...], axis=0))
    centred = (mixed - mean) * rstd
    normed = jnp.concatenate(
        [part(centred, k) * gain1 + bias1 for k in range(CHUNKS)], axis=1
    ).astype(BF16)

    span = NG * NC
    for q in ORDER:
        place = (iota((span * CAP, TOK), 0) + q * span * CAP).astype(F32)
        chosen = (place == slots[0:1, :]) | (place == slots[1:2, :])
        rows = dot(chosen.astype(F32).astype(BF16), normed, ((1,), (1,)))
        send_rows[span * q : span * (q + 1)] = rows.astype(BF16).reshape(span, CAP, FD)

        for r in range(span * q, span * (q + 1)):
            row, column = (y, x) if r % NC == 0 else (x, y)
            unless(
                jnp.logical_and(own_self, c == r) if r < NC else None,
                remote(
                    send_rows.at[r],
                    xb.at[column, q, c, row],
                    disp_s.at[r],
                    disp_r.at[q, c * NY + row],
                    expert_device(r),
                ).start,
            )

    @pl.when(own_self)
    def _():
        xb[b, 0, c, a] = send_rows[c]

    for k in range(CHUNKS):
        nat[k * LANE : (k + 1) * LANE] = part(normed, k).astype(F32).T
        for way in range(2):
            column = turned(slots[way : way + 1, k * LANE : (k + 1) * LANE])
            for j in range(EXPERTS * CAP // LANE):
                lane = (iota((LANE, LANE), 1) + j * LANE).astype(F32)
                pick[way * TOK + k * LANE : way * TOK + (k + 1) * LANE, j * LANE : (j + 1) * LANE] = (
                    (lane == column).astype(F32).astype(BF16)
                )

    relays = []

    def relay_weights(source, count):
        k = 8 + len(relays)
        from_up = source.at[up, pl.ds(0, count)]
        from_down = source.at[down, pl.ds(count, count)]
        pair = [
            remote(from_up, from_up, w_s.at[k], w_r.at[k], neighbour(down)),
            remote(from_down, from_down, w_s.at[k + 1], w_r.at[k + 1], neighbour(up)),
        ]
        for copy in pair:
            copy.start()
        relays.extend(pair)

    def wait_weights(first, last):
        for pair in weights[first:last]:
            for copy in pair:
                copy.wait_recv()

    wait_weights(0, 4)
    relay_weights(wb, HD)
    relay_weights(db, NTP * HD // 2)

    xf = {}

    def arrive(q):
        for k in range(NC * NY):
            unless(
                is_mine(q, k),
                remote(
                    send_rows.at[0],
                    xb.at[b, q, k // NY, k % NY],
                    disp_s.at[0],
                    disp_r.at[q, k],
                    here,
                ).wait_recv,
            )

        mine = xb.at[b, q]
        xf[q] = [
            remote(mine, mine, xf_s.at[0, q], xf_r.at[0, q], beside(right)),
            remote(mine, mine, xf_s.at[1, q], xf_r.at[1, q], beside(left)),
            remote(mine, mine, xf_s.at[2, q], xf_r.at[2, q], beside(across)),
        ]
        for copy in xf[q]:
            copy.start()

    def projected(group, bb):
        tiles = [
            jnp.concatenate([xb[bb, q, :, aa].reshape(GROUP, FD) for q in group], axis=0)
            for aa in range(NY)
        ]
        columns = []
        for aa in range(NY):
            start = pl.multiple_of((aa * a_step + bb * b_step) * FD, FD)
            columns.append(
                jnp.concatenate([wb[k, :, pl.ds(start, FD)] for k in range(NY)], axis=0)
            )
        return dot(
            jnp.concatenate(tiles, axis=1), jnp.concatenate(columns, axis=1), ((1,), (1,))
        )

    hx = {}

    def hidden_rows(group):
        size = len(group) * GROUP
        low = iota((size, LANE), 1) < HD
        acc[:size] = projected(group, b)
        for number, bb in enumerate((left, right, across)):
            for q in group:
                xf[q][number].wait_recv()
            acc[:size] += projected(group, bb)
        for k in range(NY // 2):
            one = acc[:size, 2 * k * LANE : (2 * k + 1) * LANE]
            two = acc[:size, (2 * k + 1) * LANE : (2 * k + 2) * LANE]
            gate = jnp.where(low, one, pltpu.roll(two, HD, 1))
            lift = jnp.where(low, pltpu.roll(one, HD, 1), two)
            hidden = (gate * jax.nn.sigmoid(gate) * lift).astype(BF16)
            for number, q in enumerate(group):
                hb[b, q, :, k * LANE : (k + 1) * LANE] = hidden[
                    number * GROUP : (number + 1) * GROUP
                ]
        for q in group:
            mine = hb.at[b, q]
            hx[q] = [
                remote(mine, mine, h_s.at[q, k], h_r.at[q, k], beside(bb))
                for k, bb in enumerate((right, left, across))
            ]
            for copy in hx[q]:
                copy.start()

    def lowered(group, bb):
        starts = [
            pl.multiple_of((aa * a_step + bb * b_step) * HD, HD) for aa in range(NY)
        ]
        blocks = [
            jnp.concatenate([db[k, pl.ds(start, HD), :] for start in starts], axis=0)
            for k in range(NY)
        ]
        rows = jnp.concatenate([hb[bb, q] for q in group], axis=0)
        return dot(rows, jnp.concatenate(blocks, axis=1))

    def give_back(group):
        size = len(group) * GROUP
        acc[:size] = lowered(group, b)
        for number, bb in enumerate((left, right, across)):
            for q in group:
                hx[q][number].wait_recv()
            acc[:size] += lowered(group, bb)
        result = acc[:size].astype(BF16)
        for number, q in enumerate(group):
            rows = result[number * GROUP : (number + 1) * GROUP]
            for aa in range(NY):
                ob[q, :, aa] = part(rows, aa).reshape(NC, CAP, FD)
            place = q * NG * NC + near * NC + c
            for k in range(NC * NY):
                unless(
                    is_mine(q, k),
                    remote(
                        ob.at[q, k // NY, k % NY],
                        rb.at[place],
                        ret_s.at[q, k],
                        ret_r.at[place],
                        source_device(q, k),
                    ).start,
                )

    first_hidden, first_down = True, True
    for step in STEPS:
        group = [int(q) for q in step[1:]]
        if step[0] == "a":
            arrive(group[0])
        elif step[0] == "g":
            if first_hidden:
                for copy in relays[:2]:
                    copy.wait_recv()
            first_hidden = False
            hidden_rows(group)
        else:
            if first_down:
                for copy in relays[2:]:
                    copy.wait_recv()
            first_down = False
            give_back(group)

    @pl.when(own_self)
    def _():
        rb[c] = ob[0, c, a]

    for back in range(1, BACK + 1):

        @pl.when(sp + back < EXPERTS)
        def _():
            remote(
                pk, pk_in.at[back - 1], pk_s.at[back - 1], pk_r.at[back - 1], here
            ).wait_send()

    @pl.when(sp + 1 < EXPERTS)
    def _():
        remote(edge, halo, halo_s, halo_r, here).wait_send()

    @pl.loop(1, NTP)
    def _(k):
        other = lax.rem(tp + k, NTP)
        remote(pg.at[tp], pg.at[tp], pg_s.at[other], pg_r.at[tp], here).wait_send()
        remote(st1.at[tp], st1.at[tp], st1_s.at[other], st1_r.at[tp], here).wait_send()

    @pl.loop(0, EXPERTS)
    def _(e):
        @pl.when(jnp.logical_not(jnp.logical_and(own_self, e == c)))
        def _():
            remote(send_rows.at[e], rb.at[0], disp_s.at[e], disp_r.at[0, 0], here).wait_send()

    for copies in weights + list(xf.values()) + list(hx.values()) + [relays]:
        for copy in copies:
            copy.wait_send()

    picked = None
    for q in ORDER:
        for r in range(NG * NC * q, NG * NC * (q + 1)):
            unless(
                jnp.logical_and(own_self, c == r) if r < NC else None,
                remote(ob.at[0, 0, 0], rb.at[r], ret_s.at[0, 0], ret_r.at[r], here).wait_recv,
            )

        group = NG * NC * CAP
        rows = dot(
            pick[:, q * group : (q + 1) * group],
            rb[NG * NC * q : NG * NC * (q + 1)].reshape(group, FD),
        )
        picked = rows if picked is None else picked + rows
    moe = []
    for k in range(CHUNKS):
        both = [turned(rweight_ref[way : way + 1, k * LANE : (k + 1) * LANE]) for way in range(2)]
        moe.append(
            rows_of(picked, k) * both[0] + rows_of(picked, CHUNKS + k) * both[1]
        )
    final = ALPHA * nat[...] + jnp.concatenate(moe, axis=0)
    for k in range(CHUNKS):
        block = rows_of(final, k).T
        st2[tp, 0:1, k * LANE : (k + 1) * LANE] = jnp.sum(block, axis=0, keepdims=True)
        st2[tp, 1:2, k * LANE : (k + 1) * LANE] = jnp.sum(block * block, axis=0, keepdims=True)

    to_plane(st2, st2_s, st2_r)

    @pl.loop(0, PIECES)
    def _(k):
        @pl.when(jnp.logical_not(jnp.logical_and(own_self, k == own_place)))
        def _():
            remote(
                ob.at[0, 0, 0],
                rb.at[0],
                ret_s.at[k // (NC * NY), lax.rem(k, NC * NY)],
                ret_r.at[0],
                here,
            ).wait_send()

    @pl.loop(1, NTP)
    def _(k):
        other = lax.rem(tp + k, NTP)
        remote(st2.at[tp], st2.at[other], st2_s.at[other], st2_r.at[other], here).wait_recv()

    mean, rstd = norm_columns(jnp.sum(st2[...], axis=0))
    for k in range(CHUNKS):
        centred = (rows_of(final, k) - turned(part(mean, k))) * turned(part(rstd, k))
        out_ref[k * LANE : (k + 1) * LANE, :] = (
            centred * gain2_ref[...] + bias2_ref[...]
        ).astype(BF16)

    @pl.loop(1, NTP)
    def _(k):
        other = lax.rem(tp + k, NTP)
        remote(st2.at[tp], st2.at[tp], st2_s.at[other], st2_r.at[tp], here).wait_send()


def body(
    pool_in,
    doc_ids,
    pool_map,
    pool_scale,
    w_out,
    gate_logit,
    residual,
    first_gain,
    first_bias,
    routes,
    route_weight,
    w_gate,
    w_up,
    w_down,
    second_gain,
    second_bias,
):
    vmem = pl.BlockSpec(memory_space=pltpu.VMEM)
    hbm = pl.BlockSpec(memory_space=pltpu.HBM)
    dma = pltpu.SemaphoreType.DMA
    args = (
        pool_in,
        doc_ids.reshape(CHUNKS, LANE),
        pool_map,
        pool_scale.reshape(1, -1),
        w_out,
        gate_logit,
        residual,
        first_gain.reshape(1, -1),
        first_bias.reshape(1, -1),
        routes.T,
        route_weight.T,
        w_gate[0].T,
        w_up[0].T,
        w_down[0],
        second_gain.reshape(1, -1),
        second_bias.reshape(1, -1),
    )
    in_specs = [hbm] * len(args)
    return pl.pallas_call(
        layer_kernel,
        out_shape=jax.ShapeDtypeStruct((TOK, FD), BF16),
        in_specs=in_specs,
        out_specs=vmem,
        scratch_shapes=[
            pltpu.VMEM((32, TOK), BF16),
            pltpu.VMEM((CHUNKS, LANE), jnp.int32),
            pltpu.VMEM((2 * NG, HD, HD), BF16),
            pltpu.VMEM((1, MIX_W), F32),
            pltpu.VMEM((MIX_W, FD), BF16),
            pltpu.VMEM((TOK, FD), BF16),
            pltpu.VMEM((TOK, FD), BF16),
            pltpu.VMEM((1, FD), F32),
            pltpu.VMEM((1, FD), F32),
            pltpu.VMEM((2, TOK), jnp.int32),
            pltpu.VMEM((2, TOK), F32),
            pltpu.VMEM((1, FD), F32),
            pltpu.VMEM((1, FD), F32),
            pltpu.VMEM((32, LANE), BF16),
            pltpu.VMEM((8, LANE), F32),
            pltpu.VMEM((BACK, 8, LANE), F32),
            pltpu.VMEM((NTP, 32, TOK), BF16),
            pltpu.VMEM((NTP, 2, TOK), F32),
            pltpu.VMEM((NTP, 2, TOK), F32),
            pltpu.VMEM((2, TOK), F32),
            pltpu.VMEM((EXPERTS, CAP, FD), BF16),
            pltpu.VMEM((NX, NG, NC, NY, CAP, FD), BF16),
            pltpu.VMEM((NY, 2 * HD, FEAT), BF16),
            pltpu.VMEM((NY, NTP * HD, FD), BF16),
            pltpu.VMEM((TOK, NY * LANE), F32),
            pltpu.VMEM((NX, NG, GROUP, NY * HD), BF16),
            pltpu.VMEM((NG, NC, NY, CAP, FD), BF16),
            pltpu.VMEM((EXPERTS, CAP, FD), BF16),
            pltpu.VMEM((2 * TOK, EXPERTS * CAP), BF16),
            pltpu.VMEM((TOK, FD), F32),
            dma((len(args),)),
            pltpu.SemaphoreType.REGULAR,
            pltpu.SemaphoreType.REGULAR,
            dma,
            dma,
            dma((BACK,)),
            dma((BACK,)),
            dma((NTP,)),
            dma((NTP,)),
            dma((NTP,)),
            dma((NTP,)),
            dma((NTP,)),
            dma((NTP,)),
            dma((EXPERTS,)),
            dma((NG, NC * NY)),
            dma((3, NG)),
            dma((3, NG)),
            dma((16,)),
            dma((16,)),
            dma((NG, 3)),
            dma((NG, 3)),
            dma((NG, NC * NY)),
            dma((EXPERTS,)),
        ],
        compiler_params=pltpu.CompilerParams(
            collective_id=0, has_side_effects=True, vmem_limit_bytes=66_000_000
        ),
        cost_estimate=pl.CostEstimate(
            flops=2_000_000_000, bytes_accessed=4_000_000, transcendentals=0
        ),
        name="layer",
    )(*args)


def solution(mesh):
    finer = Mesh(mesh.devices.reshape(NZ, NC, NY, NX), ("z", "core", "y", "x"))
    sp = ("z", "core")
    in_specs = (
        P(TP, sp),
        P(sp),
        P(),
        P(),
        P(None, TP),
        P(sp, TP),
        P(sp, TP),
        P(TP),
        P(TP),
        P(sp, None),
        P(sp, None),
        P(sp, None, TP),
        P(sp, None, TP),
        P(sp, None, TP),
        P(TP),
        P(TP),
    )
    return jax.shard_map(
        body, mesh=finer, in_specs=in_specs, out_specs=P(sp, TP), check_vma=False
    )
```

```python
import functools

import jax
import jax.numpy as jnp
from jax import lax
from jax.experimental import pallas as pl
from jax.experimental.pallas import tpu as pltpu
from jax.sharding import Mesh
from jax.sharding import PartitionSpec as P

MESH = pl.DeviceIdType.MESH
F32 = jnp.float32
BF16 = jnp.bfloat16
TP = ("y", "x")
EPS = 1e-05
ALPHA = 8.0**0.25
NZ, NC, NY, NX = 16, 2, 4, 4
NTP = NY * NX
EXPERTS = NZ * NC
CAP = 48
TOK = 384
MIX_W = 512
FEAT = 2048
FD = 128
HD = 64
LANE = 128
CHUNKS = TOK // LANE
BACK = 4
NG = NZ // NY
PIECES = NG * NC * NY
ORDER = (2, 1, 3, 0)
GROUP = NC * CAP
STEPS = ("a2", "a1", "g2", "a3", "g1", "a0", "d2", "g3", "d1", "g0", "d3", "d0")
HOPS = sorted(
    ((dy, dx) for dy in range(NY) for dx in range(NX) if dy or dx),
    key=lambda d: -min(d[0], NY - d[0]) - min(d[1], NX - d[1]),
)


def dot(a, b, dims=((1,), (0,))):
    return lax.dot_general(a, b, (dims, ((), ())), preferred_element_type=F32)


def iota(shape, dim):
    return lax.broadcasted_iota(jnp.int32, shape, dim)


def turned(row):
    return jnp.broadcast_to(row, (LANE, LANE)).T


def part(value, k):
    return value[:, k * LANE : (k + 1) * LANE]


def rows_of(value, k):
    return value[k * LANE : (k + 1) * LANE]


def remote(src, dst, send, recv, where):
    return pltpu.make_async_remote_copy(
        src_ref=src, dst_ref=dst, send_sem=send, recv_sem=recv, device_id=where, device_id_type=MESH
    )


def norm_columns(totals):
    mean = totals[0:1] / FEAT
    var = totals[1:2] / FEAT - mean * mean
    return mean, lax.rsqrt(var + EPS)


def layer_kernel(
    pool_h,
    ids_h,
    pmap_h,
    scale_h,
    wout_h,
    gate_h,
    res_h,
    gain1_h,
    bias1_h,
    routes_h,
    rweight_h,
    wg_h,
    wu_h,
    wd_h,
    gain2_h,
    bias2_h,
    out_ref,
    pool_ref,
    ids_ref,
    pmap_ref,
    scale_ref,
    wout_ref,
    gate_ref,
    res_ref,
    gain1_ref,
    bias1_ref,
    routes_ref,
    rweight_ref,
    gain2_ref,
    bias2_ref,
    halo,
    pk,
    pk_in,
    pg,
    st1,
    st2,
    slots,
    send_rows,
    xb,
    wb,
    db,
    acc,
    hb,
    ob,
    rb,
    pick,
    chosen,
    nat,
    load_sem,
    near_sem,
    far_sem,
    halo_s,
    halo_r,
    pk_s,
    pk_r,
    pg_s,
    pg_r,
    st1_s,
    st1_r,
    st2_s,
    st2_r,
    disp_s,
    disp_r,
    xf_s,
    xf_r,
    w_s,
    w_r,
    h_s,
    h_r,
    ret_s,
    ret_r,
):
    z, c, y, x = (lax.axis_index(name) for name in ("z", "core", "y", "x"))
    here = (z, c, y, x)
    sp = z * NC + c
    tp = y * NX + x
    a = jnp.where(c == 0, y, x)
    b = jnp.where(c == 0, x, y)
    a_step = jnp.where(c == 0, NX, 1)
    b_step = jnp.where(c == 0, 1, NX)
    right, left = lax.rem(b + 1, NX), lax.rem(b + NX - 1, NX)
    across = lax.rem(b + 2, NX)
    down, up = lax.rem(a + 1, NY), lax.rem(a + NY - 1, NY)
    near = lax.rem(a - 2 * z + 2 * NZ, NY)
    own_self = near == 0
    own_place = c * NY + a

    def sp_device(k):
        return (k // NC, lax.rem(k, NC), y, x)

    def plane_device(k):
        return (z, c, k // NX, lax.rem(k, NX))

    def to_plane(buffer, send, recv):
        for dy, dx in HOPS:
            yy, xx = lax.rem(y + dy, NY), lax.rem(x + dx, NX)
            other = yy * NX + xx
            remote(
                buffer.at[tp], buffer.at[tp], send.at[other], recv.at[tp], (z, c, yy, xx)
            ).start()

    def line_device(dz):
        return (lax.rem(z + dz + NZ, NZ), c, y, x)

    def turned_device(zz, cc, aa, bb):
        first = cc == 0
        return (zz, cc, jnp.where(first, aa, bb), jnp.where(first, bb, aa))

    def expert_device(r):
        ze = (z - r // NC) & (NZ - 1)
        row = (z + ze) & (NY - 1)
        return (ze, 0, row, x) if r % NC == 0 else (ze, 1, y, row)

    def unless(mine, act):
        if mine is None:
            act()
        else:
            pl.when(jnp.logical_not(mine))(lambda: act())

    def is_mine(q, k):
        return jnp.logical_and(own_self, own_place == k) if q == 0 else None

    def source_device(q, k):
        other = k % NY
        return (
            (z + near + NY * q) & (NZ - 1),
            k // NY,
            jnp.where(c == 0, other, b),
            jnp.where(c == 0, b, other),
        )

    def neighbour(aa):
        return turned_device(z, c, aa, b)

    def beside(bb):
        return turned_device(z, c, a, bb)

    def signal(sem, device):
        pl.semaphore_signal(sem, inc=1, device_id=device, device_id_type=MESH)

    loads = [
        pltpu.make_async_copy(src, dst, load_sem.at[k])
        for k, (src, dst) in enumerate(
            [
                (pool_h, pool_ref),
                (ids_h, ids_ref),
                (routes_h, routes_ref),
                (wg_h, wb.at[a, pl.ds(0, HD)]),
                (wu_h, wb.at[a, pl.ds(HD, HD)]),
                (wout_h, wout_ref),
                (gate_h, gate_ref),
                (res_h, res_ref),
                (pmap_h, pmap_ref),
                (scale_h, scale_ref),
                (gain1_h, gain1_ref),
                (bias1_h, bias1_ref),
                (wd_h, db.at[a]),
                (rweight_h, rweight_ref),
                (gain2_h, gain2_ref),
                (bias2_h, bias2_ref),
            ]
        )
    ]
    for load in loads:
        load.start()
    barrier = pltpu.get_barrier_semaphore()
    for dz in range(-2, 3):
        for other in range(NC):
            if dz:
                signal(barrier, (lax.rem(z + dz + NZ, NZ), other, y, x))
    signal(barrier, (z, 1 - c, y, x))

    @pl.loop(1, NTP)
    def _(k):
        signal(barrier, plane_device(lax.rem(tp + k, NTP)))

    loads[0].wait()
    loads[1].wait()
    ids = [ids_ref[k : k + 1, :].astype(F32) for k in range(CHUNKS)]
    pool = pool_ref[...]
    last_id = ids[CHUNKS - 1][:, LANE - 1 : LANE]
    tail = jnp.concatenate([(line == last_id).astype(F32) for line in ids], axis=1)
    tail = jnp.broadcast_to(tail, (8, TOK)).astype(BF16)
    padded = jnp.concatenate([pool, jnp.zeros((LANE - 32, TOK), BF16)], axis=0)
    padded = jnp.where(iota((LANE, TOK), 0) == 32, jnp.ones_like(padded), padded)
    sums = dot(tail, padded, ((1,), (1,)))
    line = iota((8, LANE), 0)
    packet = jnp.where(line == 0, sums, jnp.broadcast_to(last_id, (8, LANE)))
    packet = jnp.where(line == 2, jnp.broadcast_to(ids[CHUNKS - 1], (8, LANE)), packet)
    pk[...] = packet

    is_doc = x >= 2
    window = jnp.where(is_doc, 4 * TOK, jnp.left_shift(2, y))
    id_col = jnp.concatenate([turned(ids[k]) for k in range(CHUNKS)], axis=0)
    sum_own, count_own = [], []
    ones8 = jnp.ones((8, TOK), BF16)
    for k in range(CHUNKS):
        gap = iota((TOK, LANE), 1) + k * LANE - iota((TOK, LANE), 0)
        keep = (id_col == ids[k]) & (gap >= 0) & (gap < window)
        mask = keep.astype(F32).astype(BF16)
        sum_own.append(dot(pool, mask))
        count_own.append(dot(ones8, mask)[0:1])

    pl.semaphore_wait(barrier, NTP - 1 + 5 * NC - 1)

    for back in range(1, BACK + 1):

        @pl.when(sp + back < EXPERTS)
        def _():
            remote(
                pk,
                pk_in.at[back - 1],
                pk_s.at[back - 1],
                pk_r.at[back - 1],
                sp_device(sp + back),
            ).start()

    edge = pool_ref.at[:, pl.ds(TOK - LANE, LANE)]

    @pl.when(sp + 1 < EXPERTS)
    def _():
        remote(edge, halo, halo_s, halo_r, sp_device(sp + 1)).start()

    signal(near_sem, line_device(2))
    signal(near_sem, line_device(-2))

    weights = []

    def send_weights(source, first, count):
        k = 2 * len(weights)
        block = source.at[a, pl.ds(first, count)]
        pair = [
            remote(block, block, w_s.at[k], w_r.at[k], neighbour(down)),
            remote(block, block, w_s.at[k + 1], w_r.at[k + 1], neighbour(up)),
        ]
        for copy in pair:
            copy.start()
        weights.append(pair)

    loads[3].wait()
    loads[4].wait()
    send_weights(wb, 0, 32)

    for k in (2, *range(5, len(loads))):
        loads[k].wait()
    wout_t = jnp.concatenate(
        [rows_of(wout_ref[...], k).astype(F32).T for k in range(MIX_W // LANE)], axis=1
    ).astype(BF16)
    gate_t = jnp.concatenate(
        [rows_of(gate_ref[...], k).astype(F32).T for k in range(CHUNKS)], axis=1
    )
    gate_t = jax.nn.sigmoid(gate_t)
    res_t = ALPHA * jnp.concatenate(
        [rows_of(res_ref[...], k).astype(F32).T for k in range(CHUNKS)], axis=1
    )
    none = jnp.zeros((HD, HD), F32)
    maps = []
    for k in range(MIX_W // LANE):
        upper = jnp.concatenate([pmap_ref[2 * k].astype(F32), none], axis=1)
        lower = jnp.concatenate([none, pmap_ref[2 * k + 1].astype(F32)], axis=1)
        maps.append(jnp.concatenate([upper, lower], axis=0).T.astype(BF16))
    scales = [turned(part(scale_ref[...], k)) for k in range(MIX_W // LANE)]
    gain1 = turned(gain1_ref[...])
    bias1 = turned(bias1_ref[...])

    @pl.when(sp >= 1)
    def _():
        remote(edge, halo, halo_s, halo_r, here).wait_recv()

    for back in range(1, BACK + 1):

        @pl.when(sp >= back)
        def _():
            remote(
                pk, pk_in.at[back - 1], pk_s.at[back - 1], pk_r.at[back - 1], here
            ).wait_recv()

    first_id = jnp.broadcast_to(ids[0][:, 0:1], (1, LANE))
    carry = jnp.zeros((1, LANE), F32)
    for back in range(1, BACK + 1):
        found = pk_in[back - 1]
        same = (found[1:2] == first_id) & (jnp.broadcast_to(sp, (1, LANE)) >= back)
        carry = carry + jnp.where(same, found[0:1], 0.0)
    carry_col = turned(carry)
    doc_flag = is_doc.astype(F32)
    halo_on = jnp.broadcast_to(jnp.logical_and(sp >= 1, x < 2), (LANE, LANE))
    halo_ids = turned(pk_in[0][2:3])
    gap = iota((LANE, LANE), 1) + LANE - iota((LANE, LANE), 0)
    keep = (halo_ids == ids[0]) & (gap < window) & halo_on
    mask = keep.astype(F32).astype(BF16)
    halo_in = jnp.where(halo_on[0:32], halo[...].astype(F32), 0.0).astype(BF16)
    halo_sum = dot(halo_in, mask)
    halo_count = dot(ones8[:, :LANE], mask)[0:1]
    for k in range(CHUNKS):
        head = (ids[k] == first_id).astype(F32) * doc_flag
        total = sum_own[k] + carry_col[0:32] * head
        count = count_own[k] + carry_col[32:33] * head
        if k == 0:
            total = total + halo_sum
            count = count + halo_count
        pooled = total / count - part(pool, k).astype(F32)
        pg[tp, :, k * LANE : (k + 1) * LANE] = pooled.astype(BF16)

    to_plane(pg, pg_s, pg_r)

    send_weights(wb, 32, 16)
    pl.semaphore_wait(near_sem, 2)
    signal(far_sem, line_device(4))
    signal(far_sem, line_device(-4))

    expert = iota((EXPERTS, TOK), 0).astype(F32)
    routes = routes_ref[...]
    routes = ((z - routes // NC) & (NZ - 1)) * NC + (routes & (NC - 1))
    ways = [(expert == routes[k : k + 1].astype(F32)).astype(F32) for k in range(2)]
    earlier = (iota((TOK, TOK), 0) < iota((TOK, TOK), 1)).astype(F32).astype(BF16)
    rank = dot((ways[0] + ways[1]).astype(BF16), earlier) + expert * CAP
    for k in range(2):
        slots[k : k + 1, :] = jnp.sum(ways[k] * rank, axis=0, keepdims=True)
    span = NG * NC
    for q in range(NG):
        place = (iota((span * CAP, TOK), 0) + q * span * CAP).astype(F32)
        wanted = (place == slots[0:1, :]) | (place == slots[1:2, :])
        chosen[q] = wanted.astype(F32).astype(BF16)

    @pl.loop(1, NTP)
    def _(k):
        other = lax.rem(tp + k, NTP)
        remote(pg.at[tp], pg.at[other], pg_s.at[other], pg_r.at[other], here).wait_recv()

    mapped = []
    for k in range(MIX_W // LANE):
        grouped = dot(maps[k], pg[4 * k : 4 * k + 4].reshape(LANE, TOK))
        scaled = [part(grouped, j) * scales[k] for j in range(CHUNKS)]
        mapped.append(jnp.concatenate(scaled, axis=1).astype(BF16))
    mixed = res_t + dot(wout_t, jnp.concatenate(mapped, axis=0)) * gate_t
    st1[tp, 0:1] = jnp.sum(mixed, axis=0, keepdims=True)
    st1[tp, 1:2] = jnp.sum(mixed * mixed, axis=0, keepdims=True)

    pl.semaphore_wait(far_sem, 2)

    to_plane(st1, st1_s, st1_r)

    send_weights(wb, 48, 80)
    send_weights(db, 0, NTP * HD)

    @pl.loop(1, NTP)
    def _(k):
        other = lax.rem(tp + k, NTP)
        remote(st1.at[tp], st1.at[other], st1_s.at[other], st1_r.at[other], here).wait_recv()

    mean, rstd = norm_columns(jnp.sum(st1[...], axis=0))
    centred = (mixed - mean) * rstd
    normed = jnp.concatenate(
        [part(centred, k) * gain1 + bias1 for k in range(CHUNKS)], axis=1
    ).astype(BF16)

    for q in ORDER:
        rows = dot(chosen[q], normed, ((1,), (1,)))
        send_rows[span * q : span * (q + 1)] = rows.astype(BF16).reshape(span, CAP, FD)

        for r in range(span * q, span * (q + 1)):
            row, column = (y, x) if r % NC == 0 else (x, y)
            unless(
                jnp.logical_and(own_self, c == r) if r < NC else None,
                remote(
                    send_rows.at[r],
                    xb.at[column, q, c, row],
                    disp_s.at[r],
                    disp_r.at[q, c * NY + row],
                    expert_device(r),
                ).start,
            )

    @pl.when(own_self)
    def _():
        xb[b, 0, c, a] = send_rows[c]

    for k in range(CHUNKS):
        nat[k * LANE : (k + 1) * LANE] = part(normed, k).astype(F32).T
        for way in range(2):
            column = turned(slots[way : way + 1, k * LANE : (k + 1) * LANE])
            for j in range(EXPERTS * CAP // LANE):
                lane = (iota((LANE, LANE), 1) + j * LANE).astype(F32)
                pick[way * TOK + k * LANE : way * TOK + (k + 1) * LANE, j * LANE : (j + 1) * LANE] = (
                    (lane == column).astype(F32).astype(BF16)
                )

    relays = []

    def relay_weights(source, count):
        k = 8 + len(relays)
        from_up = source.at[up, pl.ds(0, count)]
        from_down = source.at[down, pl.ds(count, count)]
        pair = [
            remote(from_up, from_up, w_s.at[k], w_r.at[k], neighbour(down)),
            remote(from_down, from_down, w_s.at[k + 1], w_r.at[k + 1], neighbour(up)),
        ]
        for copy in pair:
            copy.start()
        relays.extend(pair)

    def wait_weights(first, last):
        for pair in weights[first:last]:
            for copy in pair:
                copy.wait_recv()

    wait_weights(0, 4)
    relay_weights(wb, HD)
    relay_weights(db, NTP * HD // 2)

    xf = {}

    def arrive(q):
        for k in range(NC * NY):
            unless(
                is_mine(q, k),
                remote(
                    send_rows.at[0],
                    xb.at[b, q, k // NY, k % NY],
                    disp_s.at[0],
                    disp_r.at[q, k],
                    here,
                ).wait_recv,
            )

        mine = xb.at[b, q]
        xf[q] = [
            remote(mine, mine, xf_s.at[0, q], xf_r.at[0, q], beside(right)),
            remote(mine, mine, xf_s.at[1, q], xf_r.at[1, q], beside(left)),
            remote(mine, mine, xf_s.at[2, q], xf_r.at[2, q], beside(across)),
        ]
        for copy in xf[q]:
            copy.start()

    def projected(group, bb):
        tiles = [
            jnp.concatenate([xb[bb, q, :, aa].reshape(GROUP, FD) for q in group], axis=0)
            for aa in range(NY)
        ]
        columns = []
        for aa in range(NY):
            start = pl.multiple_of((aa * a_step + bb * b_step) * FD, FD)
            columns.append(
                jnp.concatenate([wb[k, :, pl.ds(start, FD)] for k in range(NY)], axis=0)
            )
        return dot(
            jnp.concatenate(tiles, axis=1), jnp.concatenate(columns, axis=1), ((1,), (1,))
        )

    hx = {}

    def hidden_rows(group):
        size = len(group) * GROUP
        low = iota((size, LANE), 1) < HD
        acc[:size] = projected(group, b)
        for number, bb in enumerate((left, right, across)):
            for q in group:
                xf[q][number].wait_recv()
            acc[:size] += projected(group, bb)
        for k in range(NY // 2):
            one = acc[:size, 2 * k * LANE : (2 * k + 1) * LANE]
            two = acc[:size, (2 * k + 1) * LANE : (2 * k + 2) * LANE]
            gate = jnp.where(low, one, pltpu.roll(two, HD, 1))
            lift = jnp.where(low, pltpu.roll(one, HD, 1), two)
            hidden = (gate * jax.nn.sigmoid(gate) * lift).astype(BF16)
            for number, q in enumerate(group):
                hb[b, q, :, k * LANE : (k + 1) * LANE] = hidden[
                    number * GROUP : (number + 1) * GROUP
                ]
        for q in group:
            mine = hb.at[b, q]
            hx[q] = [
                remote(mine, mine, h_s.at[q, k], h_r.at[q, k], beside(bb))
                for k, bb in enumerate((right, left, across))
            ]
            for copy in hx[q]:
                copy.start()

    def lowered(group, bb):
        starts = [
            pl.multiple_of((aa * a_step + bb * b_step) * HD, HD) for aa in range(NY)
        ]
        blocks = [
            jnp.concatenate([db[k, pl.ds(start, HD), :] for start in starts], axis=0)
            for k in range(NY)
        ]
        rows = jnp.concatenate([hb[bb, q] for q in group], axis=0)
        return dot(rows, jnp.concatenate(blocks, axis=1))

    def give_back(group):
        size = len(group) * GROUP
        acc[:size] = lowered(group, b)
        for number, bb in enumerate((left, right, across)):
            for q in group:
                hx[q][number].wait_recv()
            acc[:size] += lowered(group, bb)
        result = acc[:size].astype(BF16)
        for number, q in enumerate(group):
            rows = result[number * GROUP : (number + 1) * GROUP]
            for aa in range(NY):
                ob[q, :, aa] = part(rows, aa).reshape(NC, CAP, FD)
            place = q * NG * NC + near * NC + c
            for k in range(NC * NY):
                unless(
                    is_mine(q, k),
                    remote(
                        ob.at[q, k // NY, k % NY],
                        rb.at[place],
                        ret_s.at[q, k],
                        ret_r.at[place],
                        source_device(q, k),
                    ).start,
                )

    first_hidden, first_down = True, True
    for step in STEPS:
        group = [int(q) for q in step[1:]]
        if step[0] == "a":
            arrive(group[0])
        elif step[0] == "g":
            if first_hidden:
                for copy in relays[:2]:
                    copy.wait_recv()
            first_hidden = False
            hidden_rows(group)
        else:
            if first_down:
                for copy in relays[2:]:
                    copy.wait_recv()
            first_down = False
            give_back(group)

    @pl.when(own_self)
    def _():
        rb[c] = ob[0, c, a]

    for back in range(1, BACK + 1):

        @pl.when(sp + back < EXPERTS)
        def _():
            remote(
                pk, pk_in.at[back - 1], pk_s.at[back - 1], pk_r.at[back - 1], here
            ).wait_send()

    @pl.when(sp + 1 < EXPERTS)
    def _():
        remote(edge, halo, halo_s, halo_r, here).wait_send()

    @pl.loop(1, NTP)
    def _(k):
        other = lax.rem(tp + k, NTP)
        remote(pg.at[tp], pg.at[tp], pg_s.at[other], pg_r.at[tp], here).wait_send()
        remote(st1.at[tp], st1.at[tp], st1_s.at[other], st1_r.at[tp], here).wait_send()

    @pl.loop(0, EXPERTS)
    def _(e):
        @pl.when(jnp.logical_not(jnp.logical_and(own_self, e == c)))
        def _():
            remote(send_rows.at[e], rb.at[0], disp_s.at[e], disp_r.at[0, 0], here).wait_send()

    for copies in weights + list(xf.values()) + list(hx.values()) + [relays]:
        for copy in copies:
            copy.wait_send()

    picked = None
    for q in ORDER:
        for r in range(NG * NC * q, NG * NC * (q + 1)):
            unless(
                jnp.logical_and(own_self, c == r) if r < NC else None,
                remote(ob.at[0, 0, 0], rb.at[r], ret_s.at[0, 0], ret_r.at[r], here).wait_recv,
            )

        group = NG * NC * CAP
        rows = dot(
            pick[:, q * group : (q + 1) * group],
            rb[NG * NC * q : NG * NC * (q + 1)].reshape(group, FD),
        )
        picked = rows if picked is None else picked + rows
    moe = []
    for k in range(CHUNKS):
        both = [turned(rweight_ref[way : way + 1, k * LANE : (k + 1) * LANE]) for way in range(2)]
        moe.append(
            rows_of(picked, k) * both[0] + rows_of(picked, CHUNKS + k) * both[1]
        )
    final = ALPHA * nat[...] + jnp.concatenate(moe, axis=0)
    for k in range(CHUNKS):
        block = rows_of(final, k).T
        st2[tp, 0:1, k * LANE : (k + 1) * LANE] = jnp.sum(block, axis=0, keepdims=True)
        st2[tp, 1:2, k * LANE : (k + 1) * LANE] = jnp.sum(block * block, axis=0, keepdims=True)

    to_plane(st2, st2_s, st2_r)

    @pl.loop(0, PIECES)
    def _(k):
        @pl.when(jnp.logical_not(jnp.logical_and(own_self, k == own_place)))
        def _():
            remote(
                ob.at[0, 0, 0],
                rb.at[0],
                ret_s.at[k // (NC * NY), lax.rem(k, NC * NY)],
                ret_r.at[0],
                here,
            ).wait_send()

    @pl.loop(1, NTP)
    def _(k):
        other = lax.rem(tp + k, NTP)
        remote(st2.at[tp], st2.at[other], st2_s.at[other], st2_r.at[other], here).wait_recv()

    mean, rstd = norm_columns(jnp.sum(st2[...], axis=0))
    for k in range(CHUNKS):
        centred = (rows_of(final, k) - turned(part(mean, k))) * turned(part(rstd, k))
        out_ref[k * LANE : (k + 1) * LANE, :] = (
            centred * gain2_ref[...] + bias2_ref[...]
        ).astype(BF16)

    @pl.loop(1, NTP)
    def _(k):
        other = lax.rem(tp + k, NTP)
        remote(st2.at[tp], st2.at[tp], st2_s.at[other], st2_r.at[tp], here).wait_send()


def body(
    pool_in,
    doc_ids,
    pool_map,
    pool_scale,
    w_out,
    gate_logit,
    residual,
    first_gain,
    first_bias,
    routes,
    route_weight,
    w_gate,
    w_up,
    w_down,
    second_gain,
    second_bias,
):
    vmem = pl.BlockSpec(memory_space=pltpu.VMEM)
    hbm = pl.BlockSpec(memory_space=pltpu.HBM)
    dma = pltpu.SemaphoreType.DMA
    args = (
        pool_in,
        doc_ids.reshape(CHUNKS, LANE),
        pool_map,
        pool_scale.reshape(1, -1),
        w_out,
        gate_logit,
        residual,
        first_gain.reshape(1, -1),
        first_bias.reshape(1, -1),
        routes.T,
        route_weight.T,
        w_gate[0].T,
        w_up[0].T,
        w_down[0],
        second_gain.reshape(1, -1),
        second_bias.reshape(1, -1),
    )
    in_specs = [hbm] * len(args)
    return pl.pallas_call(
        layer_kernel,
        out_shape=jax.ShapeDtypeStruct((TOK, FD), BF16),
        in_specs=in_specs,
        out_specs=vmem,
        scratch_shapes=[
            pltpu.VMEM((32, TOK), BF16),
            pltpu.VMEM((CHUNKS, LANE), jnp.int32),
            pltpu.VMEM((2 * NG, HD, HD), BF16),
            pltpu.VMEM((1, MIX_W), F32),
            pltpu.VMEM((MIX_W, FD), BF16),
            pltpu.VMEM((TOK, FD), BF16),
            pltpu.VMEM((TOK, FD), BF16),
            pltpu.VMEM((1, FD), F32),
            pltpu.VMEM((1, FD), F32),
            pltpu.VMEM((2, TOK), jnp.int32),
            pltpu.VMEM((2, TOK), F32),
            pltpu.VMEM((1, FD), F32),
            pltpu.VMEM((1, FD), F32),
            pltpu.VMEM((32, LANE), BF16),
            pltpu.VMEM((8, LANE), F32),
            pltpu.VMEM((BACK, 8, LANE), F32),
            pltpu.VMEM((NTP, 32, TOK), BF16),
            pltpu.VMEM((NTP, 2, TOK), F32),
            pltpu.VMEM((NTP, 2, TOK), F32),
            pltpu.VMEM((2, TOK), F32),
            pltpu.VMEM((EXPERTS, CAP, FD), BF16),
            pltpu.VMEM((NX, NG, NC, NY, CAP, FD), BF16),
            pltpu.VMEM((NY, 2 * HD, FEAT), BF16),
            pltpu.VMEM((NY, NTP * HD, FD), BF16),
            pltpu.VMEM((TOK, NY * LANE), F32),
            pltpu.VMEM((NX, NG, GROUP, NY * HD), BF16),
            pltpu.VMEM((NG, NC, NY, CAP, FD), BF16),
            pltpu.VMEM((EXPERTS, CAP, FD), BF16),
            pltpu.VMEM((2 * TOK, EXPERTS * CAP), BF16),
            pltpu.VMEM((NG, EXPERTS * CAP // NG, TOK), BF16),
            pltpu.VMEM((TOK, FD), F32),
            dma((len(args),)),
            pltpu.SemaphoreType.REGULAR,
            pltpu.SemaphoreType.REGULAR,
            dma,
            dma,
            dma((BACK,)),
            dma((BACK,)),
            dma((NTP,)),
            dma((NTP,)),
            dma((NTP,)),
            dma((NTP,)),
            dma((NTP,)),
            dma((NTP,)),
            dma((EXPERTS,)),
            dma((NG, NC * NY)),
            dma((3, NG)),
            dma((3, NG)),
            dma((16,)),
            dma((16,)),
            dma((NG, 3)),
            dma((NG, 3)),
            dma((NG, NC * NY)),
            dma((EXPERTS,)),
        ],
        compiler_params=pltpu.CompilerParams(
            collective_id=0, has_side_effects=True, vmem_limit_bytes=66_000_000
        ),
        cost_estimate=pl.CostEstimate(
            flops=2_000_000_000, bytes_accessed=4_000_000, transcendentals=0
        ),
        name="layer",
    )(*args)


def solution(mesh):
    finer = Mesh(mesh.devices.reshape(NZ, NC, NY, NX), ("z", "core", "y", "x"))
    sp = ("z", "core")
    in_specs = (
        P(TP, sp),
        P(sp),
        P(),
        P(),
        P(None, TP),
        P(sp, TP),
        P(sp, TP),
        P(TP),
        P(TP),
        P(sp, None),
        P(sp, None),
        P(sp, None, TP),
        P(sp, None, TP),
        P(sp, None, TP),
        P(TP),
        P(TP),
    )
    return jax.shard_map(
        body, mesh=finer, in_specs=in_specs, out_specs=P(sp, TP), check_vma=False
    )
```

```python
import functools

import jax
import jax.numpy as jnp
from jax import lax
from jax.experimental import pallas as pl
from jax.experimental.pallas import tpu as pltpu
from jax.sharding import Mesh
from jax.sharding import PartitionSpec as P

MESH = pl.DeviceIdType.MESH
F32 = jnp.float32
BF16 = jnp.bfloat16
TP = ("y", "x")
EPS = 1e-05
ALPHA = 8.0**0.25
NZ, NC, NY, NX = 16, 2, 4, 4
NTP = NY * NX
EXPERTS = NZ * NC
CAP = 48
TOK = 384
MIX_W = 512
FEAT = 2048
FD = 128
HD = 64
LANE = 128
CHUNKS = TOK // LANE
BACK = 4
NG = NZ // NY
PIECES = NG * NC * NY
ORDER = (2, 1, 3, 0)
GROUP = NC * CAP
STEPS = ("a2", "a1", "g2", "a3", "g1", "a0", "d2", "g3", "d1", "g0", "d3", "d0")
HOPS = sorted(
    ((dy, dx) for dy in range(NY) for dx in range(NX) if dy or dx),
    key=lambda d: -min(d[0], NY - d[0]) - min(d[1], NX - d[1]),
)


def dot(a, b, dims=((1,), (0,))):
    return lax.dot_general(a, b, (dims, ((), ())), preferred_element_type=F32)


def iota(shape, dim):
    return lax.broadcasted_iota(jnp.int32, shape, dim)


def turned(row):
    return jnp.broadcast_to(row, (LANE, LANE)).T


def part(value, k):
    return value[:, k * LANE : (k + 1) * LANE]


def rows_of(value, k):
    return value[k * LANE : (k + 1) * LANE]


def remote(src, dst, send, recv, where):
    return pltpu.make_async_remote_copy(
        src_ref=src, dst_ref=dst, send_sem=send, recv_sem=recv, device_id=where, device_id_type=MESH
    )


def norm_columns(totals):
    mean = totals[0:1] / FEAT
    var = totals[1:2] / FEAT - mean * mean
    return mean, lax.rsqrt(var + EPS)


def layer_kernel(
    pool_h,
    ids_h,
    pmap_h,
    scale_h,
    wout_h,
    gate_h,
    res_h,
    gain1_h,
    bias1_h,
    routes_h,
    rweight_h,
    wg_h,
    wu_h,
    wd_h,
    gain2_h,
    bias2_h,
    out_ref,
    pool_ref,
    ids_ref,
    pmap_ref,
    scale_ref,
    wout_ref,
    gate_ref,
    res_ref,
    gain1_ref,
    bias1_ref,
    routes_ref,
    rweight_ref,
    gain2_ref,
    bias2_ref,
    halo,
    pk,
    pk_in,
    pg,
    st1,
    st2,
    slots,
    send_rows,
    xb,
    wb,
    db,
    acc,
    hb,
    ob,
    rb,
    pick,
    chosen,
    nat,
    load_sem,
    near_sem,
    far_sem,
    halo_s,
    halo_r,
    pk_s,
    pk_r,
    pg_s,
    pg_r,
    st1_s,
    st1_r,
    st2_s,
    st2_r,
    disp_s,
    disp_r,
    xf_s,
    xf_r,
    w_s,
    w_r,
    h_s,
    h_r,
    ret_s,
    ret_r,
):
    z, c, y, x = (lax.axis_index(name) for name in ("z", "core", "y", "x"))
    here = (z, c, y, x)
    sp = z * NC + c
    tp = y * NX + x
    a = jnp.where(c == 0, y, x)
    b = jnp.where(c == 0, x, y)
    a_step = jnp.where(c == 0, NX, 1)
    b_step = jnp.where(c == 0, 1, NX)
    right, left = lax.rem(b + 1, NX), lax.rem(b + NX - 1, NX)
    across = lax.rem(b + 2, NX)
    down, up = lax.rem(a + 1, NY), lax.rem(a + NY - 1, NY)
    near = lax.rem(a - 2 * z + 2 * NZ, NY)
    own_self = near == 0
    own_place = c * NY + a

    def sp_device(k):
        return (k // NC, lax.rem(k, NC), y, x)

    def plane_device(k):
        return (z, c, k // NX, lax.rem(k, NX))

    def to_plane(buffer, send, recv):
        for dy, dx in HOPS:
            yy, xx = lax.rem(y + dy, NY), lax.rem(x + dx, NX)
            other = yy * NX + xx
            remote(
                buffer.at[tp], buffer.at[tp], send.at[other], recv.at[tp], (z, c, yy, xx)
            ).start()

    def line_device(dz):
        return (lax.rem(z + dz + NZ, NZ), c, y, x)

    def turned_device(zz, cc, aa, bb):
        first = cc == 0
        return (zz, cc, jnp.where(first, aa, bb), jnp.where(first, bb, aa))

    def expert_device(r):
        ze = (z - r // NC) & (NZ - 1)
        row = (z + ze) & (NY - 1)
        return (ze, 0, row, x) if r % NC == 0 else (ze, 1, y, row)

    def unless(mine, act):
        if mine is None:
            act()
        else:
            pl.when(jnp.logical_not(mine))(lambda: act())

    def is_mine(q, k):
        return jnp.logical_and(own_self, own_place == k) if q == 0 else None

    def source_device(q, k):
        other = k % NY
        return (
            (z + near + NY * q) & (NZ - 1),
            k // NY,
            jnp.where(c == 0, other, b),
            jnp.where(c == 0, b, other),
        )

    def neighbour(aa):
        return turned_device(z, c, aa, b)

    def beside(bb):
        return turned_device(z, c, a, bb)

    def signal(sem, device):
        pl.semaphore_signal(sem, inc=1, device_id=device, device_id_type=MESH)

    loads = [
        pltpu.make_async_copy(src, dst, load_sem.at[k])
        for k, (src, dst) in enumerate(
            [
                (pool_h, pool_ref),
                (ids_h, ids_ref),
                (routes_h, routes_ref),
                (wg_h, wb.at[a, pl.ds(0, HD)]),
                (wu_h, wb.at[a, pl.ds(HD, HD)]),
                (wout_h, wout_ref),
                (gate_h, gate_ref),
                (res_h, res_ref),
                (pmap_h, pmap_ref),
                (scale_h, scale_ref),
                (gain1_h, gain1_ref),
                (bias1_h, bias1_ref),
                (wd_h, db.at[a]),
                (rweight_h, rweight_ref),
                (gain2_h, gain2_ref),
                (bias2_h, bias2_ref),
            ]
        )
    ]
    barrier = pltpu.get_barrier_semaphore()
    for dz in range(-2, 3):
        for other in range(NC):
            if dz:
                signal(barrier, (lax.rem(z + dz + NZ, NZ), other, y, x))
    signal(barrier, (z, 1 - c, y, x))

    @pl.loop(1, NTP)
    def _(k):
        signal(barrier, plane_device(lax.rem(tp + k, NTP)))

    for load in loads:
        load.start()

    loads[0].wait()
    loads[1].wait()
    ids = [ids_ref[k : k + 1, :].astype(F32) for k in range(CHUNKS)]
    pool = pool_ref[...]
    last_id = ids[CHUNKS - 1][:, LANE - 1 : LANE]
    tail = jnp.concatenate([(line == last_id).astype(F32) for line in ids], axis=1)
    tail = jnp.broadcast_to(tail, (8, TOK)).astype(BF16)
    padded = jnp.concatenate([pool, jnp.zeros((LANE - 32, TOK), BF16)], axis=0)
    padded = jnp.where(iota((LANE, TOK), 0) == 32, jnp.ones_like(padded), padded)
    sums = dot(tail, padded, ((1,), (1,)))
    line = iota((8, LANE), 0)
    packet = jnp.where(line == 0, sums, jnp.broadcast_to(last_id, (8, LANE)))
    packet = jnp.where(line == 2, jnp.broadcast_to(ids[CHUNKS - 1], (8, LANE)), packet)
    pk[...] = packet

    is_doc = x >= 2
    window = jnp.where(is_doc, 4 * TOK, jnp.left_shift(2, y))
    id_col = jnp.concatenate([turned(ids[k]) for k in range(CHUNKS)], axis=0)
    sum_own, count_own = [], []
    ones8 = jnp.ones((8, TOK), BF16)
    for k in range(CHUNKS):
        gap = iota((TOK, LANE), 1) + k * LANE - iota((TOK, LANE), 0)
        keep = (id_col == ids[k]) & (gap >= 0) & (gap < window)
        mask = keep.astype(F32).astype(BF16)
        sum_own.append(dot(pool, mask))
        count_own.append(dot(ones8, mask)[0:1])

    pl.semaphore_wait(barrier, NTP - 1 + 5 * NC - 1)

    for back in range(1, BACK + 1):

        @pl.when(sp + back < EXPERTS)
        def _():
            remote(
                pk,
                pk_in.at[back - 1],
                pk_s.at[back - 1],
                pk_r.at[back - 1],
                sp_device(sp + back),
            ).start()

    edge = pool_ref.at[:, pl.ds(TOK - LANE, LANE)]

    @pl.when(sp + 1 < EXPERTS)
    def _():
        remote(edge, halo, halo_s, halo_r, sp_device(sp + 1)).start()

    signal(near_sem, line_device(2))
    signal(near_sem, line_device(-2))

    weights = []

    def send_weights(source, first, count):
        k = 2 * len(weights)
        block = source.at[a, pl.ds(first, count)]
        pair = [
            remote(block, block, w_s.at[k], w_r.at[k], neighbour(down)),
            remote(block, block, w_s.at[k + 1], w_r.at[k + 1], neighbour(up)),
        ]
        for copy in pair:
            copy.start()
        weights.append(pair)

    loads[3].wait()
    loads[4].wait()
    send_weights(wb, 0, 32)

    for k in (2, *range(5, len(loads))):
        loads[k].wait()
    wout_t = jnp.concatenate(
        [rows_of(wout_ref[...], k).astype(F32).T for k in range(MIX_W // LANE)], axis=1
    ).astype(BF16)
    gate_t = jnp.concatenate(
        [rows_of(gate_ref[...], k).astype(F32).T for k in range(CHUNKS)], axis=1
    )
    gate_t = jax.nn.sigmoid(gate_t)
    res_t = ALPHA * jnp.concatenate(
        [rows_of(res_ref[...], k).astype(F32).T for k in range(CHUNKS)], axis=1
    )
    none = jnp.zeros((HD, HD), F32)
    maps = []
    for k in range(MIX_W // LANE):
        upper = jnp.concatenate([pmap_ref[2 * k].astype(F32), none], axis=1)
        lower = jnp.concatenate([none, pmap_ref[2 * k + 1].astype(F32)], axis=1)
        maps.append(jnp.concatenate([upper, lower], axis=0).T.astype(BF16))
    scales = [turned(part(scale_ref[...], k)) for k in range(MIX_W // LANE)]
    gain1 = turned(gain1_ref[...])
    bias1 = turned(bias1_ref[...])

    @pl.when(sp >= 1)
    def _():
        remote(edge, halo, halo_s, halo_r, here).wait_recv()

    for back in range(1, BACK + 1):

        @pl.when(sp >= back)
        def _():
            remote(
                pk, pk_in.at[back - 1], pk_s.at[back - 1], pk_r.at[back - 1], here
            ).wait_recv()

    first_id = jnp.broadcast_to(ids[0][:, 0:1], (1, LANE))
    carry = jnp.zeros((1, LANE), F32)
    for back in range(1, BACK + 1):
        found = pk_in[back - 1]
        same = (found[1:2] == first_id) & (jnp.broadcast_to(sp, (1, LANE)) >= back)
        carry = carry + jnp.where(same, found[0:1], 0.0)
    carry_col = turned(carry)
    doc_flag = is_doc.astype(F32)
    halo_on = jnp.broadcast_to(jnp.logical_and(sp >= 1, x < 2), (LANE, LANE))
    halo_ids = turned(pk_in[0][2:3])
    gap = iota((LANE, LANE), 1) + LANE - iota((LANE, LANE), 0)
    keep = (halo_ids == ids[0]) & (gap < window) & halo_on
    mask = keep.astype(F32).astype(BF16)
    halo_in = jnp.where(halo_on[0:32], halo[...].astype(F32), 0.0).astype(BF16)
    halo_sum = dot(halo_in, mask)
    halo_count = dot(ones8[:, :LANE], mask)[0:1]
    for k in range(CHUNKS):
        head = (ids[k] == first_id).astype(F32) * doc_flag
        total = sum_own[k] + carry_col[0:32] * head
        count = count_own[k] + carry_col[32:33] * head
        if k == 0:
            total = total + halo_sum
            count = count + halo_count
        pooled = total / count - part(pool, k).astype(F32)
        pg[tp, :, k * LANE : (k + 1) * LANE] = pooled.astype(BF16)

    to_plane(pg, pg_s, pg_r)

    send_weights(wb, 32, 16)
    pl.semaphore_wait(near_sem, 2)
    signal(far_sem, line_device(4))
    signal(far_sem, line_device(-4))

    expert = iota((EXPERTS, TOK), 0).astype(F32)
    routes = routes_ref[...]
    routes = ((z - routes // NC) & (NZ - 1)) * NC + (routes & (NC - 1))
    ways = [(expert == routes[k : k + 1].astype(F32)).astype(F32) for k in range(2)]
    earlier = (iota((TOK, TOK), 0) < iota((TOK, TOK), 1)).astype(F32).astype(BF16)
    rank = dot((ways[0] + ways[1]).astype(BF16), earlier) + expert * CAP
    for k in range(2):
        slots[k : k + 1, :] = jnp.sum(ways[k] * rank, axis=0, keepdims=True)
    span = NG * NC
    for q in range(NG):
        place = (iota((span * CAP, TOK), 0) + q * span * CAP).astype(F32)
        wanted = (place == slots[0:1, :]) | (place == slots[1:2, :])
        chosen[q] = wanted.astype(F32).astype(BF16)

    @pl.loop(1, NTP)
    def _(k):
        other = lax.rem(tp + k, NTP)
        remote(pg.at[tp], pg.at[other], pg_s.at[other], pg_r.at[other], here).wait_recv()

    mapped = []
    for k in range(MIX_W // LANE):
        grouped = dot(maps[k], pg[4 * k : 4 * k + 4].reshape(LANE, TOK))
        scaled = [part(grouped, j) * scales[k] for j in range(CHUNKS)]
        mapped.append(jnp.concatenate(scaled, axis=1).astype(BF16))
    mixed = res_t + dot(wout_t, jnp.concatenate(mapped, axis=0)) * gate_t
    st1[tp, 0:1] = jnp.sum(mixed, axis=0, keepdims=True)
    st1[tp, 1:2] = jnp.sum(mixed * mixed, axis=0, keepdims=True)

    pl.semaphore_wait(far_sem, 2)

    to_plane(st1, st1_s, st1_r)

    send_weights(wb, 48, 80)
    send_weights(db, 0, NTP * HD)

    @pl.loop(1, NTP)
    def _(k):
        other = lax.rem(tp + k, NTP)
        remote(st1.at[tp], st1.at[other], st1_s.at[other], st1_r.at[other], here).wait_recv()

    mean, rstd = norm_columns(jnp.sum(st1[...], axis=0))
    centred = (mixed - mean) * rstd
    normed = jnp.concatenate(
        [part(centred, k) * gain1 + bias1 for k in range(CHUNKS)], axis=1
    ).astype(BF16)

    for q in ORDER:
        rows = dot(chosen[q], normed, ((1,), (1,)))
        send_rows[span * q : span * (q + 1)] = rows.astype(BF16).reshape(span, CAP, FD)

        for r in range(span * q, span * (q + 1)):
            row, column = (y, x) if r % NC == 0 else (x, y)
            unless(
                jnp.logical_and(own_self, c == r) if r < NC else None,
                remote(
                    send_rows.at[r],
                    xb.at[column, q, c, row],
                    disp_s.at[r],
                    disp_r.at[q, c * NY + row],
                    expert_device(r),
                ).start,
            )

    @pl.when(own_self)
    def _():
        xb[b, 0, c, a] = send_rows[c]

    for k in range(CHUNKS):
        nat[k * LANE : (k + 1) * LANE] = part(normed, k).astype(F32).T
        for way in range(2):
            column = turned(slots[way : way + 1, k * LANE : (k + 1) * LANE])
            for j in range(EXPERTS * CAP // LANE):
                lane = (iota((LANE, LANE), 1) + j * LANE).astype(F32)
                pick[way * TOK + k * LANE : way * TOK + (k + 1) * LANE, j * LANE : (j + 1) * LANE] = (
                    (lane == column).astype(F32).astype(BF16)
                )

    relays = []

    def relay_weights(source, count):
        k = 8 + len(relays)
        from_up = source.at[up, pl.ds(0, count)]
        from_down = source.at[down, pl.ds(count, count)]
        pair = [
            remote(from_up, from_up, w_s.at[k], w_r.at[k], neighbour(down)),
            remote(from_down, from_down, w_s.at[k + 1], w_r.at[k + 1], neighbour(up)),
        ]
        for copy in pair:
            copy.start()
        relays.extend(pair)

    def wait_weights(first, last):
        for pair in weights[first:last]:
            for copy in pair:
                copy.wait_recv()

    wait_weights(0, 4)
    relay_weights(wb, HD)
    relay_weights(db, NTP * HD // 2)

    xf = {}

    def arrive(q):
        for k in range(NC * NY):
            unless(
                is_mine(q, k),
                remote(
                    send_rows.at[0],
                    xb.at[b, q, k // NY, k % NY],
                    disp_s.at[0],
                    disp_r.at[q, k],
                    here,
                ).wait_recv,
            )

        mine = xb.at[b, q]
        xf[q] = [
            remote(mine, mine, xf_s.at[0, q], xf_r.at[0, q], beside(right)),
            remote(mine, mine, xf_s.at[1, q], xf_r.at[1, q], beside(left)),
            remote(mine, mine, xf_s.at[2, q], xf_r.at[2, q], beside(across)),
        ]
        for copy in xf[q]:
            copy.start()

    def projected(group, bb):
        tiles = [
            jnp.concatenate([xb[bb, q, :, aa].reshape(GROUP, FD) for q in group], axis=0)
            for aa in range(NY)
        ]
        columns = []
        for aa in range(NY):
            start = pl.multiple_of((aa * a_step + bb * b_step) * FD, FD)
            columns.append(
                jnp.concatenate([wb[k, :, pl.ds(start, FD)] for k in range(NY)], axis=0)
            )
        return dot(
            jnp.concatenate(tiles, axis=1), jnp.concatenate(columns, axis=1), ((1,), (1,))
        )

    hx = {}

    def hidden_rows(group):
        size = len(group) * GROUP
        low = iota((size, LANE), 1) < HD
        acc[:size] = projected(group, b)
        for number, bb in enumerate((left, right, across)):
            for q in group:
                xf[q][number].wait_recv()
            acc[:size] += projected(group, bb)
        for k in range(NY // 2):
            one = acc[:size, 2 * k * LANE : (2 * k + 1) * LANE]
            two = acc[:size, (2 * k + 1) * LANE : (2 * k + 2) * LANE]
            gate = jnp.where(low, one, pltpu.roll(two, HD, 1))
            lift = jnp.where(low, pltpu.roll(one, HD, 1), two)
            hidden = (gate * jax.nn.sigmoid(gate) * lift).astype(BF16)
            for number, q in enumerate(group):
                hb[b, q, :, k * LANE : (k + 1) * LANE] = hidden[
                    number * GROUP : (number + 1) * GROUP
                ]
        for q in group:
            mine = hb.at[b, q]
            hx[q] = [
                remote(mine, mine, h_s.at[q, k], h_r.at[q, k], beside(bb))
                for k, bb in enumerate((right, left, across))
            ]
            for copy in hx[q]:
                copy.start()

    def lowered(group, bb):
        starts = [
            pl.multiple_of((aa * a_step + bb * b_step) * HD, HD) for aa in range(NY)
        ]
        blocks = [
            jnp.concatenate([db[k, pl.ds(start, HD), :] for start in starts], axis=0)
            for k in range(NY)
        ]
        rows = jnp.concatenate([hb[bb, q] for q in group], axis=0)
        return dot(rows, jnp.concatenate(blocks, axis=1))

    def give_back(group):
        size = len(group) * GROUP
        acc[:size] = lowered(group, b)
        for number, bb in enumerate((left, right, across)):
            for q in group:
                hx[q][number].wait_recv()
            acc[:size] += lowered(group, bb)
        result = acc[:size].astype(BF16)
        for number, q in enumerate(group):
            rows = result[number * GROUP : (number + 1) * GROUP]
            for aa in range(NY):
                ob[q, :, aa] = part(rows, aa).reshape(NC, CAP, FD)
            place = q * NG * NC + near * NC + c
            for k in range(NC * NY):
                unless(
                    is_mine(q, k),
                    remote(
                        ob.at[q, k // NY, k % NY],
                        rb.at[place],
                        ret_s.at[q, k],
                        ret_r.at[place],
                        source_device(q, k),
                    ).start,
                )

    first_hidden, first_down = True, True
    for step in STEPS:
        group = [int(q) for q in step[1:]]
        if step[0] == "a":
            arrive(group[0])
        elif step[0] == "g":
            if first_hidden:
                for copy in relays[:2]:
                    copy.wait_recv()
            first_hidden = False
            hidden_rows(group)
        else:
            if first_down:
                for copy in relays[2:]:
                    copy.wait_recv()
            first_down = False
            give_back(group)

    @pl.when(own_self)
    def _():
        rb[c] = ob[0, c, a]

    for back in range(1, BACK + 1):

        @pl.when(sp + back < EXPERTS)
        def _():
            remote(
                pk, pk_in.at[back - 1], pk_s.at[back - 1], pk_r.at[back - 1], here
            ).wait_send()

    @pl.when(sp + 1 < EXPERTS)
    def _():
        remote(edge, halo, halo_s, halo_r, here).wait_send()

    @pl.loop(1, NTP)
    def _(k):
        other = lax.rem(tp + k, NTP)
        remote(pg.at[tp], pg.at[tp], pg_s.at[other], pg_r.at[tp], here).wait_send()
        remote(st1.at[tp], st1.at[tp], st1_s.at[other], st1_r.at[tp], here).wait_send()

    @pl.loop(0, EXPERTS)
    def _(e):
        @pl.when(jnp.logical_not(jnp.logical_and(own_self, e == c)))
        def _():
            remote(send_rows.at[e], rb.at[0], disp_s.at[e], disp_r.at[0, 0], here).wait_send()

    for copies in weights + list(xf.values()) + list(hx.values()) + [relays]:
        for copy in copies:
            copy.wait_send()

    picked = None
    for q in ORDER:
        for r in range(NG * NC * q, NG * NC * (q + 1)):
            unless(
                jnp.logical_and(own_self, c == r) if r < NC else None,
                remote(ob.at[0, 0, 0], rb.at[r], ret_s.at[0, 0], ret_r.at[r], here).wait_recv,
            )

        group = NG * NC * CAP
        rows = dot(
            pick[:, q * group : (q + 1) * group],
            rb[NG * NC * q : NG * NC * (q + 1)].reshape(group, FD),
        )
        picked = rows if picked is None else picked + rows
    moe = []
    for k in range(CHUNKS):
        both = [turned(rweight_ref[way : way + 1, k * LANE : (k + 1) * LANE]) for way in range(2)]
        moe.append(
            rows_of(picked, k) * both[0] + rows_of(picked, CHUNKS + k) * both[1]
        )
    final = ALPHA * nat[...] + jnp.concatenate(moe, axis=0)
    for k in range(CHUNKS):
        block = rows_of(final, k).T
        st2[tp, 0:1, k * LANE : (k + 1) * LANE] = jnp.sum(block, axis=0, keepdims=True)
        st2[tp, 1:2, k * LANE : (k + 1) * LANE] = jnp.sum(block * block, axis=0, keepdims=True)

    to_plane(st2, st2_s, st2_r)

    @pl.loop(0, PIECES)
    def _(k):
        @pl.when(jnp.logical_not(jnp.logical_and(own_self, k == own_place)))
        def _():
            remote(
                ob.at[0, 0, 0],
                rb.at[0],
                ret_s.at[k // (NC * NY), lax.rem(k, NC * NY)],
                ret_r.at[0],
                here,
            ).wait_send()

    @pl.loop(1, NTP)
    def _(k):
        other = lax.rem(tp + k, NTP)
        remote(st2.at[tp], st2.at[other], st2_s.at[other], st2_r.at[other], here).wait_recv()

    mean, rstd = norm_columns(jnp.sum(st2[...], axis=0))
    for k in range(CHUNKS):
        centred = (rows_of(final, k) - turned(part(mean, k))) * turned(part(rstd, k))
        out_ref[k * LANE : (k + 1) * LANE, :] = (
            centred * gain2_ref[...] + bias2_ref[...]
        ).astype(BF16)

    @pl.loop(1, NTP)
    def _(k):
        other = lax.rem(tp + k, NTP)
        remote(st2.at[tp], st2.at[tp], st2_s.at[other], st2_r.at[tp], here).wait_send()


def body(
    pool_in,
    doc_ids,
    pool_map,
    pool_scale,
    w_out,
    gate_logit,
    residual,
    first_gain,
    first_bias,
    routes,
    route_weight,
    w_gate,
    w_up,
    w_down,
    second_gain,
    second_bias,
):
    vmem = pl.BlockSpec(memory_space=pltpu.VMEM)
    hbm = pl.BlockSpec(memory_space=pltpu.HBM)
    dma = pltpu.SemaphoreType.DMA
    args = (
        pool_in,
        doc_ids.reshape(CHUNKS, LANE),
        pool_map,
        pool_scale.reshape(1, -1),
        w_out,
        gate_logit,
        residual,
        first_gain.reshape(1, -1),
        first_bias.reshape(1, -1),
        routes.T,
        route_weight.T,
        w_gate[0].T,
        w_up[0].T,
        w_down[0],
        second_gain.reshape(1, -1),
        second_bias.reshape(1, -1),
    )
    in_specs = [hbm] * len(args)
    return pl.pallas_call(
        layer_kernel,
        out_shape=jax.ShapeDtypeStruct((TOK, FD), BF16),
        in_specs=in_specs,
        out_specs=vmem,
        scratch_shapes=[
            pltpu.VMEM((32, TOK), BF16),
            pltpu.VMEM((CHUNKS, LANE), jnp.int32),
            pltpu.VMEM((2 * NG, HD, HD), BF16),
            pltpu.VMEM((1, MIX_W), F32),
            pltpu.VMEM((MIX_W, FD), BF16),
            pltpu.VMEM((TOK, FD), BF16),
            pltpu.VMEM((TOK, FD), BF16),
            pltpu.VMEM((1, FD), F32),
            pltpu.VMEM((1, FD), F32),
            pltpu.VMEM((2, TOK), jnp.int32),
            pltpu.VMEM((2, TOK), F32),
            pltpu.VMEM((1, FD), F32),
            pltpu.VMEM((1, FD), F32),
            pltpu.VMEM((32, LANE), BF16),
            pltpu.VMEM((8, LANE), F32),
            pltpu.VMEM((BACK, 8, LANE), F32),
            pltpu.VMEM((NTP, 32, TOK), BF16),
            pltpu.VMEM((NTP, 2, TOK), F32),
            pltpu.VMEM((NTP, 2, TOK), F32),
            pltpu.VMEM((2, TOK), F32),
            pltpu.VMEM((EXPERTS, CAP, FD), BF16),
            pltpu.VMEM((NX, NG, NC, NY, CAP, FD), BF16),
            pltpu.VMEM((NY, 2 * HD, FEAT), BF16),
            pltpu.VMEM((NY, NTP * HD, FD), BF16),
            pltpu.VMEM((TOK, NY * LANE), F32),
            pltpu.VMEM((NX, NG, GROUP, NY * HD), BF16),
            pltpu.VMEM((NG, NC, NY, CAP, FD), BF16),
            pltpu.VMEM((EXPERTS, CAP, FD), BF16),
            pltpu.VMEM((2 * TOK, EXPERTS * CAP), BF16),
            pltpu.VMEM((NG, EXPERTS * CAP // NG, TOK), BF16),
            pltpu.VMEM((TOK, FD), F32),
            dma((len(args),)),
            pltpu.SemaphoreType.REGULAR,
            pltpu.SemaphoreType.REGULAR,
            dma,
            dma,
            dma((BACK,)),
            dma((BACK,)),
            dma((NTP,)),
            dma((NTP,)),
            dma((NTP,)),
            dma((NTP,)),
            dma((NTP,)),
            dma((NTP,)),
            dma((EXPERTS,)),
            dma((NG, NC * NY)),
            dma((3, NG)),
            dma((3, NG)),
            dma((16,)),
            dma((16,)),
            dma((NG, 3)),
            dma((NG, 3)),
            dma((NG, NC * NY)),
            dma((EXPERTS,)),
        ],
        compiler_params=pltpu.CompilerParams(
            collective_id=0, has_side_effects=True, vmem_limit_bytes=66_000_000
        ),
        cost_estimate=pl.CostEstimate(
            flops=2_000_000_000, bytes_accessed=4_000_000, transcendentals=0
        ),
        name="layer",
    )(*args)


def solution(mesh):
    finer = Mesh(mesh.devices.reshape(NZ, NC, NY, NX), ("z", "core", "y", "x"))
    sp = ("z", "core")
    in_specs = (
        P(TP, sp),
        P(sp),
        P(),
        P(),
        P(None, TP),
        P(sp, TP),
        P(sp, TP),
        P(TP),
        P(TP),
        P(sp, None),
        P(sp, None),
        P(sp, None, TP),
        P(sp, None, TP),
        P(sp, None, TP),
        P(TP),
        P(TP),
    )
    return jax.shard_map(
        body, mesh=finer, in_specs=in_specs, out_specs=P(sp, TP), check_vma=False
    )
```
